256 devices in a mesh: sp: 64 (over z, x, core), tp: 4 (over y).
Axes of the slice: x: 4, y: 4, z: 8, core: 2. Of those that a mesh axis runs over, the one named last changes fastest.
Arguments:
- residual_in: bfloat16 [16384, 2048], P('sp', 'tp'), may hold values from -6 to 6
- conv_input: bfloat16 [16384, 512], P('sp', 'tp'), may hold values from -6 to 6
- outer_gate: bfloat16 [16384, 512], P('sp', 'tp'), may hold values from -6 to 6
- inner_gate: bfloat16 [16384, 512], P('sp', 'tp'), may hold values from -6 to 6
- documents: int32 [16384], P('sp'), may hold values from 0 to 31, as said below
- conv_taps: float32 [3, 512], P(None, 'tp'), may hold values from -3 to 3
- mixer_gain: float32 [512], replicated, may hold values from 0.1 to 1.9
- output_weight: bfloat16 [512, 2048], P(None, 'tp'), may hold values from -0.25 to 0.25
- ffn_gain: float32 [2048], P('tp'), may hold values from 0.1 to 1.9
- routes: int32 [16384, 2], P('sp'), may hold values from 0 to 63, all different within a row; in each aligned block of 256 rows (0 to 255, 256 to 511, ...) at most 16 rows name the same one
- route_weights: float32 [16384, 2], P('sp'), may hold values from 0.1 to 0.9
- expert_gate: bfloat16 [64, 2048, 3584], P('sp', None, 'tp'), may hold values from -0.125 to 0.125
- expert_up: bfloat16 [64, 2048, 3584], P('sp', None, 'tp'), may hold values from -0.125 to 0.125
- expert_down: bfloat16 [64, 3584, 2048], P('sp', 'tp'), may hold values from -0.09375 to 0.09375
Outputs:
- layer_out: bfloat16 [16384, 2048], P('sp', 'tp')
The draws below stay inside these ranges and needn't reach their ends.
Inputs may be any that keep to these rules, and one draw needn't show every extreme that they name: Document numbers never fall along the positions, and each of the 32 documents occurs. Every document has 256 to 768 positions, and one has exactly 768. `routes`: the two experts of a position differ. Among the 256 positions of one index of sp no expert is named more than 16 times, a bound that some block reaches.
All inputs are finite; a program needn't handle non-finite values.
Results may differ from the reference program's by a relative error of at most 0.0058.
Values may be sent and summed in bfloat16 or wider, within the bound.
A program may use at most 64 MiB of HBM per device.

```python
import math
import jax
import jax.numpy as jnp
import numpy as np
from jax import lax

D = 2048
CH = 512
FE = 3584
TOK_DEV = 256
TOKENS = 16384
EXPERTS = 64
CAP = 16
SEGS = 32
N_SP = 64
N_TP = 4


def draw_documents(key, part):
    half = TOK_DEV // 2
    pick_key = jax.random.fold_in(key, 11)
    shift_key = jax.random.fold_in(key, 23)
    longest = jax.random.randint(pick_key, (), 1, SEGS - 1, dtype=jnp.int32)
    jitter = jax.random.randint(shift_key, (SEGS - 1,), -half, half + 1, dtype=jnp.int32)
    number = jnp.arange(1, SEGS, dtype=jnp.int32)
    jitter = jnp.where(number == longest, -half, jitter)
    jitter = jnp.where(number == longest + 1, half, jitter)
    starts = number * (2 * TOK_DEV) + jitter
    places = jnp.arange(TOKENS, dtype=jnp.int32)
    return jnp.sum((places[:, None] >= starts[None, :]).astype(jnp.int32), axis=1).astype(jnp.int32)


def shard_levels(rng, extent, cuts, low, largest):
    def one(axis_at, blocks):
        steps = jax.random.uniform(jax.random.fold_in(jax.random.fold_in(rng, 6), axis_at), (blocks,), jnp.float32, low / len(cuts), largest / len(cuts))
        return jnp.repeat(jnp.exp(steps), extent[axis_at] // blocks).reshape((-1,) + (1,) * (len(extent) - axis_at - 1))

    gain = one(*cuts[0])
    for cut in cuts[1:]:
        gain = gain * one(*cut)
    return gain


def deal_out(key, own, number, rows, amount, top, bound, lean):
    sequence = jax.random.permutation(key, amount)
    heavy_load, usual = shares(amount, rows * top, bound, lean, True), shares(amount, rows * top, bound, lean, False)
    places = jnp.arange(amount)

    def named(tallies, offset_by):
        used = int((tallies > 0).sum())
        fixed = max(1, used // 4)
        shifted = fixed + (places - fixed + offset_by * (used - fixed)) % max(1, amount - fixed)
        return jnp.zeros((amount,), jnp.int32).at[sequence[jnp.where(places < fixed, places, shifted)]].set(jnp.asarray(tallies, jnp.int32))

    tallies = jnp.where(number % 4 == 0, named(heavy_load, number // 4), named(usual, number - number // 4 - 1))
    mixed = jax.random.permutation(jax.random.fold_in(own, 3), amount)
    source_of, taker = mixed[0:amount // 2 * 2:2], mixed[1:amount // 2 * 2:2]
    slack = jnp.minimum(tallies[source_of] - 1, bound - tallies[taker]) // 2
    slack = jnp.where((source_of == sequence[0]) | (taker == sequence[0]) | (tallies[taker] == 0), 0, jnp.maximum(slack, 0))
    shifted = jax.random.randint(jax.random.fold_in(own, 4), (amount // 2,), 0, 1 << 20) % (slack + 1)
    tallies = tallies.at[source_of].add(-shifted).at[taker].add(shifted)
    labels = jnp.searchsorted(jnp.cumsum(tallies), jnp.arange(rows * top), side="right").astype(jnp.int32)
    grid = labels.reshape(top, rows).T
    grid = grid[jax.random.permutation(jax.random.fold_in(own, 1), rows)]
    offset_by = jax.random.randint(jax.random.fold_in(own, 2), (rows, 1), 0, top)
    return jnp.take_along_axis(grid, (jnp.arange(top)[None, :] + offset_by) % top, axis=1)


def shares(count, total, limit, skew, full):
    portions = [(1 << 20) // math.isqrt(rank ** skew) + 1 for rank in range(1, count + 1)]
    largest = limit if full else min(limit, max(-(-total // count), total * portions[0] // sum(portions)))
    least = 1 if total - largest >= count - 1 else 0
    holding, rest = [largest] + [least] * (count - 1), total - largest - least * (count - 1)
    while rest > 0:
        movable = [i for i in range(1, count) if holding[i] < largest] or [i for i in range(1, count) if holding[i] < limit]
        whole, left = sum([portions[i] for i in movable]), rest
        for i in movable:
            extra = min(limit - holding[i], max(1, left * portions[i] // whole), rest)
            holding[i] = holding[i] + extra
            rest = rest - extra
    return np.array(holding)


def centred(rng, dims, deviation, limit, pieces=(), kind=jnp.bfloat16):
    array = deviation * jax.random.normal(rng, dims, jnp.float32)
    if pieces:
        array = array * shard_levels(rng, dims, pieces, -0.22, 0.18)
    return jnp.clip(array, -limit, limit).astype(kind)


def setup_inputs(seed: int = 0) -> dict:
    seeds = jax.random.split(jax.random.key(seed), 15)
    residual_in = centred(seeds[0], (TOKENS, D), 1.0, 6.0, ((0, 64), (1, 4)))
    conv_input = centred(seeds[1], (TOKENS, CH), 1.0, 6.0, ((0, 64), (1, 4)))
    outer_gate = centred(seeds[2], (TOKENS, CH), 1.0, 6.0, ((0, 64), (1, 4)))
    inner_gate = centred(seeds[3], (TOKENS, CH), 1.0, 6.0, ((0, 64), (1, 4)))
    documents = draw_documents(jax.random.fold_in(seeds[14], 71), 0)
    conv_taps = centred(seeds[5], (3, CH), 0.6, 3.0, ((1, 4),), jnp.float32)
    mixer_gain = jnp.clip(1.0 + 0.18 * jax.random.normal(seeds[6], (CH,), jnp.float32), 0.1, 1.9)
    output_weight = centred(seeds[7], (CH, D), CH ** -0.5, 0.25, ((1, 4),))
    ffn_gain = jnp.clip(1.0 + 0.18 * jax.random.normal(seeds[8], (D,), jnp.float32), 0.1, 1.9)
    routes_keys = jax.random.split(jax.random.fold_in(seeds[9], 1), TOKENS // TOK_DEV)
    routes_turns = jax.random.permutation(jax.random.fold_in(seeds[9], 3), TOKENS // TOK_DEV)
    routes = jax.vmap(lambda own, number: deal_out(jax.random.fold_in(seeds[9], 2), own, number, TOK_DEV, EXPERTS, 2, CAP, 1))(routes_keys, routes_turns).reshape((TOKENS, 2))
    route_weights = jnp.clip(0.1 + 0.79999997 * jax.random.uniform(seeds[10], (TOKENS, 2), jnp.float32) ** shard_levels(seeds[10], (TOKENS, 2), ((0, 64),), -0.2, 0.2), 0.1, 0.9)
    expert_gate = centred(seeds[11], (EXPERTS, D, FE), D ** -0.5, 0.125, ((0, 64), (2, 4)))
    expert_up = centred(seeds[12], (EXPERTS, D, FE), D ** -0.5, 0.125, ((0, 64), (2, 4)))
    expert_down = centred(seeds[13], (EXPERTS, FE, D), FE ** -0.5, 0.09375, ((0, 64), (1, 4)))
    return {"residual_in": residual_in, "conv_input": conv_input, "outer_gate": outer_gate, "inner_gate": inner_gate, "documents": documents, "conv_taps": conv_taps, "mixer_gain": mixer_gain, "output_weight": output_weight, "ffn_gain": ffn_gain, "routes": routes, "route_weights": route_weights, "expert_gate": expert_gate, "expert_up": expert_up, "expert_down": expert_down}


EPS = 1e-06

def slot_tables(routes, experts, capacity):
    tokens = routes.shape[0]
    flattened = routes.reshape(-1)
    onehot = (flattened[:, None] == jnp.arange(experts, dtype=jnp.int32)[None, :]).astype(jnp.int32)
    earlier = jnp.cumsum(onehot, axis=0) - onehot
    position_in = lax.optimization_barrier(jnp.sum(earlier * onehot, axis=1))
    target = flattened * capacity + position_in
    owners = jnp.full((experts * capacity,), tokens, jnp.int32).at[target].set(jnp.arange(2 * tokens, dtype=jnp.int32) // 2)
    return (target.astype(jnp.int32), owners)

def reference(residual_in, conv_input, outer_gate, inner_gate, documents, conv_taps, mixer_gain, output_weight, ffn_gain, routes, route_weights, expert_gate, expert_up, expert_down):
    conv_value = (inner_gate.astype(jnp.float32) * conv_input.astype(jnp.float32)).astype(jnp.bfloat16)
    values = conv_value.astype(jnp.float32)
    zero_row = jnp.zeros((1, CH), jnp.float32)
    back_one = jnp.concatenate([zero_row, values[:-1]], axis=0)
    back_two = jnp.concatenate([zero_row, zero_row, values[:-2]], axis=0)
    minus = jnp.full((1,), -1, jnp.int32)
    doc_one = jnp.concatenate([minus, documents[:-1]], axis=0)
    doc_two = jnp.concatenate([minus, minus, documents[:-2]], axis=0)
    same_one = (doc_one == documents).astype(jnp.float32)[:, None]
    same_two = (doc_two == documents).astype(jnp.float32)[:, None]
    conv_sum = conv_taps[2] * values + conv_taps[1] * back_one * same_one + conv_taps[0] * back_two * same_two
    mixed = (outer_gate.astype(jnp.float32) * conv_sum).astype(jnp.bfloat16)
    mixed_f = mixed.astype(jnp.float32)
    mix_scale = lax.rsqrt(lax.optimization_barrier(jnp.mean(mixed_f * mixed_f, axis=1)) + EPS)
    mix_scaled = (mixed_f * mixer_gain).astype(jnp.bfloat16)
    projected = jnp.dot(mix_scaled, output_weight, preferred_element_type=jnp.float32)
    hidden_state = residual_in.astype(jnp.float32) + projected * mix_scale[:, None]
    feature_scale = lax.rsqrt(lax.optimization_barrier(jnp.mean(hidden_state * hidden_state, axis=1)) + EPS)
    normed = (hidden_state * feature_scale[:, None] * ffn_gain).astype(jnp.bfloat16)
    blocks = routes.reshape(N_SP, TOK_DEV, 2)
    target, owners = jax.vmap(lambda r: slot_tables(r, EXPERTS, CAP))(blocks)
    offsets = (jnp.arange(N_SP, dtype=jnp.int32) * TOK_DEV)[:, None]
    global_owner = jnp.where(owners == TOK_DEV, TOKENS, owners + offsets).astype(jnp.int32)
    expert_index = global_owner.reshape(N_SP, EXPERTS, CAP).transpose(1, 0, 2).reshape(EXPERTS, N_SP * CAP)
    padded = jnp.concatenate([normed, jnp.zeros((1, D), jnp.bfloat16)], axis=0)
    quarter = FE // N_TP

    def one_expert(inputs):
        gate_w, up_w, down_w, index_rows = inputs
        rows = padded[index_rows]
        gate = jnp.dot(rows, gate_w, preferred_element_type=jnp.float32)
        upper = jnp.dot(rows, up_w, preferred_element_type=jnp.float32)
        act = (jax.nn.silu(gate) * upper).astype(jnp.bfloat16)
        total = jnp.zeros((rows.shape[0], D), jnp.float32)
        for block in range(N_TP):
            partial_out = jnp.dot(act[:, block * quarter:(block + 1) * quarter], down_w[block * quarter:(block + 1) * quarter], preferred_element_type=jnp.float32)
            total = total + partial_out.astype(jnp.bfloat16).astype(jnp.float32)
        return total.astype(jnp.bfloat16)
    expert_rows = lax.map(one_expert, (expert_gate, expert_up, expert_down, expert_index))
    expert_of = target // CAP
    slot_of = target % CAP
    global_slot = expert_of * (N_SP * CAP) + (jnp.arange(N_SP, dtype=jnp.int32) * CAP)[:, None] + slot_of
    picked = expert_rows.reshape(EXPERTS * N_SP * CAP, D)[global_slot.reshape(-1)]
    picked = picked.astype(jnp.float32).reshape(TOKENS, 2, D)
    routed = lax.optimization_barrier(jnp.sum(picked * route_weights[:, :, None], axis=1))
    return (hidden_state + routed).astype(jnp.bfloat16)
```

```python
import functools

import jax
import jax.numpy as jnp
from jax import lax
from jax.experimental import pallas as pl
from jax.experimental.pallas import tpu as pltpu
from jax.sharding import PartitionSpec as P

EPS = 1e-06
CORES = 2
NX = 4
MESH = pl.DeviceIdType.MESH
F32 = jnp.float32
BF16 = jnp.bfloat16


def layer_kernel(
    nsp,
    ntp,
    cap,
    res_h,
    ci_h,
    og_h,
    ig_h,
    doc_h,
    taps_h,
    mg_h,
    ow_h,
    fg_h,
    rt_h,
    rw_h,
    wg_h,
    wu_h,
    wd_h,
    out_ref,
    res,
    ci,
    og,
    ig,
    doc,
    taps,
    mg,
    ow,
    fg,
    rt,
    rw,
    wg,
    wu,
    wd,
    rows8,
    cols8,
    joined,
    docj,
    halo_out,
    halo_in,
    mix,
    ss,
    hid,
    perm,
    outgo,
    xin,
    act,
    part,
    ra,
    rb,
    fl,
    fr,
    ret,
    ret_in,
    load_sem,
    halo_sem,
    mix_s,
    mix_r,
    ss_s,
    ss_r,
    disp_s,
    disp_r,
    ag_s,
    ag_r,
    rs_s,
    rs_r,
    ret_s,
    ret_r,
):
    sp = lax.axis_index("sp")
    tp = lax.axis_index("tp")
    nz = nsp // (NX * CORES)
    zpos = sp // (NX * CORES)
    xpos = (sp // CORES) % NX
    cpos = sp % CORES
    tokens, features = res.shape
    channels = ci.shape[1]
    group = nz * CORES * cap
    half = group // 2
    pair = CORES * cap
    left = lax.rem(tp + ntp - 1, ntp)
    right = lax.rem(tp + 1, ntp)
    opposite = lax.rem(tp + 2, ntp)

    barrier = pltpu.get_barrier_semaphore()

    def greet(step, carry):
        pl.semaphore_signal(
            barrier,
            inc=1,
            device_id=(lax.rem(sp + step, nsp), tp),
            device_id_type=MESH,
        )
        return carry

    lax.fori_loop(1, nsp, greet, 0)
    for d in range(1, ntp):
        pl.semaphore_signal(
            barrier, inc=1, device_id=(sp, lax.rem(tp + d, ntp)), device_id_type=MESH
        )

    pairs = (
        (rt_h, rt),
        (doc_h, doc),
        (rw_h, rw),
        (ci_h, ci),
        (ig_h, ig),
        (og_h, og),
        (taps_h, taps),
        (mg_h, mg),
        (ow_h, ow),
        (res_h, res),
        (fg_h, fg),
        (wg_h.at[0], wg),
        (wu_h.at[0], wu),
        (wd_h.at[0], wd),
    )
    loads = [
        pltpu.make_async_copy(src, dst, load_sem.at[i]) for i, (src, dst) in enumerate(pairs)
    ]
    for load in loads:
        load.start()

    for i in range(3):
        loads[i].wait()
    experts_iota = lax.broadcasted_iota(jnp.int32, (nsp, tokens), 0)
    first = (experts_iota == rt[0:1, :]).astype(F32)
    second = (experts_iota == rt[1:2, :]).astype(F32)
    named = (first + second).astype(BF16)
    before = (
        lax.broadcasted_iota(jnp.int32, (tokens, tokens), 0)
        < lax.broadcasted_iota(jnp.int32, (tokens, tokens), 1)
    ).astype(F32).astype(BF16)
    earlier = jnp.dot(named, before, preferred_element_type=F32)
    slots = earlier + (experts_iota * cap).astype(F32)
    rows8[0:1, :] = doc[...].astype(F32)
    rows8[1:2, :] = jnp.sum(first * slots, axis=0, keepdims=True)
    rows8[2:3, :] = jnp.sum(second * slots, axis=0, keepdims=True)
    rows8[3:5, :] = rw[...]
    rows8[5:8, :] = jnp.zeros((3, tokens), F32)
    cols8[...] = jnp.transpose(rows8[...])

    loads[3].wait()
    loads[4].wait()
    value = (ig[...].astype(F32) * ci[...].astype(F32)).astype(BF16).astype(F32)
    joined[8:, :] = value
    docj[8:, :] = jnp.broadcast_to(cols8[:, 0:1], (tokens, channels))
    halo_out[0:8, :] = value[tokens - 8 :, :]
    halo_out[8:16, :] = jnp.broadcast_to(cols8[tokens - 8 :, 0:1], (8, channels))

    pl.semaphore_wait(barrier, nsp + ntp - 2)
    halo = pltpu.make_async_remote_copy(
        src_ref=halo_out,
        dst_ref=halo_in,
        send_sem=halo_sem.at[0],
        recv_sem=halo_sem.at[1],
        device_id=(lax.rem(sp + 1, nsp), tp),
        device_id_type=MESH,
    )
    halo.start()

    line = lax.broadcasted_iota(jnp.int32, (group, tokens), 0)
    spread = (line // pair) * (NX * pair) + lax.rem(line, pair)
    for j in range(NX):
        slot = (spread + lax.rem(xpos + j, NX) * pair).astype(F32)
        hit = (slot == rows8[1:2, :]) | (slot == rows8[2:3, :])
        perm[j] = hit.astype(F32).astype(BF16)

    for i in range(5, 7):
        loads[i].wait()
    halo.wait()
    joined[0:8, :] = halo_in[0:8, :]
    docj[0:8, :] = jnp.where(sp == 0, -1.0, halo_in[8:16, :])
    docs_now = docj[8:, :]
    same_one = (docj[7 : tokens + 7, :] == docs_now).astype(F32)
    same_two = (docj[6 : tokens + 6, :] == docs_now).astype(F32)
    conv_sum = (
        taps[2:3, :] * joined[8:, :]
        + taps[1:2, :] * joined[7 : tokens + 7, :] * same_one
        + taps[0:1, :] * joined[6 : tokens + 6, :] * same_two
    )
    mix[tp] = (og[...].astype(F32) * conv_sum).astype(BF16)

    def to_tp(buffer, send, recv):
        copies = []
        for d in (1, ntp - 1, *range(2, ntp - 1)):
            copies.append(
                pltpu.make_async_remote_copy(
                    src_ref=buffer.at[tp],
                    dst_ref=buffer.at[tp],
                    send_sem=send.at[d - 1],
                    recv_sem=recv.at[d - 1],
                    device_id=(sp, lax.rem(tp + d, ntp)),
                    device_id_type=MESH,
                )
            )
        for copy in copies:
            copy.start()
        return copies

    mix_copies = to_tp(mix, mix_s, mix_r)
    for i in range(7, 11):
        loads[i].wait()
    for copy in mix_copies:
        copy.wait()
    pieces = jnp.concatenate([mix[q] for q in range(ntp)], axis=1).astype(F32)
    squares = jnp.sum(pieces * pieces, axis=1, keepdims=True)
    mix_scale = lax.rsqrt(squares / (channels * ntp) + EPS)
    scaled = (pieces * mg[...]).astype(BF16)
    projected = jnp.dot(scaled, ow[...], preferred_element_type=F32)
    hidden = res[...].astype(F32) + projected * mix_scale
    hid[...] = hidden
    power = hidden * hidden
    folded = power[:, 0:128]
    for k in range(1, features // 128):
        folded = folded + power[:, k * 128 : (k + 1) * 128]
    ss[tp] = jnp.broadcast_to(
        jnp.sum(jnp.transpose(folded), axis=0, keepdims=True), (8, tokens)
    )
    ss_copies = to_tp(ss, ss_s, ss_r)
    for copy in ss_copies:
        copy.wait()
    total = ss[0]
    for q in range(1, ntp):
        total = total + ss[q]
    scale = jnp.transpose(lax.rsqrt(total / (features * ntp) + EPS))[:, 0:1]
    normed = (hid[...] * scale * fg[...]).astype(BF16)

    mine = pl.multiple_of((zpos * CORES + cpos) * cap, cap)

    def exchange(src, dst, send, recv, j, xx):
        def one(zz, cc):
            at = pl.multiple_of((zz * CORES + cc) * cap, cap)
            pltpu.make_async_remote_copy(
                src_ref=src.at[j, pl.ds(at, cap)],
                dst_ref=dst(j, mine),
                send_sem=send.at[j],
                recv_sem=recv.at[j],
                device_id=((zz * NX + xx) * CORES + cc, tp),
                device_id_type=MESH,
            ).start()

        def far(i, carry):
            h = i // 2 + 1
            k = jnp.where(lax.rem(i, 2) == 0, h, nz - h)
            zz = lax.rem(zpos + k, nz)
            for cc in range(CORES):
                one(zz, cc)
            return carry

        lax.fori_loop(0, nz - 1, far, 0)
        if j == 0:
            one(zpos, 1 - cpos)
        else:
            for cc in range(CORES):
                one(zpos, cc)

    def rows_of(j):
        return group - cap if j == 0 else group

    for j in range(NX):
        outgo[j] = jnp.dot(perm[j], normed, preferred_element_type=F32).astype(BF16)
        if j == 0:
            xin[tp, 0, pl.ds(mine, cap), :] = outgo[0, pl.ds(mine, cap), :]
        exchange(
            outgo,
            lambda j, at: xin.at[tp, j, pl.ds(at, cap)],
            disp_s,
            disp_r,
            j,
            lax.rem(xpos + j, NX),
        )

    def tp_copy(src, dst, send, recv, to):
        return pltpu.make_async_remote_copy(
            src_ref=src,
            dst_ref=dst,
            send_sem=send,
            recv_sem=recv,
            device_id=(sp, to),
            device_id_type=MESH,
        )

    upper = pl.ds(0, half)
    lower = pl.ds(half, half)

    def got(ref, sem):
        pltpu.make_async_copy(ref, ref, sem).wait()

    def own(j):
        got(xin.at[tp, j, pl.ds(0, rows_of(j))], disp_r.at[j])
        tp_copy(xin.at[tp, j], xin.at[tp, j], ag_s.at[0, j], ag_r.at[0, j], right).start()
        tp_copy(xin.at[tp, j], xin.at[tp, j], ag_s.at[1, j], ag_r.at[1, j], left).start()

    def forward(j):
        got(xin.at[left, j], ag_r.at[0, j])
        ref = xin.at[left, j, upper]
        tp_copy(ref, ref, ag_s.at[2, j], ag_r.at[2, j], right).start()
        got(xin.at[right, j], ag_r.at[1, j])
        ref = xin.at[right, j, lower]
        tp_copy(ref, ref, ag_s.at[3, j], ag_r.at[3, j], left).start()

    hidden_units = wg.shape[1]
    tile = 128
    wide = 256
    per_q = features // wide

    def experts(j):
        got(xin.at[opposite, j, upper], ag_r.at[2, j])
        got(xin.at[opposite, j, lower], ag_r.at[3, j])

        def up_tile(n, carry):
            at = pl.ds(pl.multiple_of(n * tile, tile), tile)
            rows = jnp.concatenate([xin[q, j] for q in range(ntp)], axis=1)
            both = jnp.concatenate([wg[:, at], wu[:, at]], axis=1)
            made = jnp.dot(rows, both, preferred_element_type=F32)
            gate = made[:, :tile]
            act[:, at] = (jax.nn.silu(gate) * made[:, tile:]).astype(BF16)
            return carry

        lax.fori_loop(0, hidden_units // tile, up_tile, 0)
        for q in range(ntp):
            for k in range(per_q):
                cols = slice(q * features + k * wide, q * features + (k + 1) * wide)
                part[j, q, :, k * wide : (k + 1) * wide] = jnp.dot(
                    act[...], wd[:, cols], preferred_element_type=F32
                ).astype(BF16)
        tp_copy(part.at[j, opposite, upper], ra.at[j], rs_s.at[0, j], rs_r.at[0, j], right).start()
        tp_copy(part.at[j, opposite, lower], rb.at[j], rs_s.at[1, j], rs_r.at[1, j], left).start()
        tp_copy(
            part.at[j, right, lower], fl.at[j, lower], rs_s.at[2, j], rs_r.at[2, j], right
        ).start()
        tp_copy(
            part.at[j, left, upper], fr.at[j, upper], rs_s.at[3, j], rs_r.at[3, j], left
        ).start()

    def add_on(j):
        got(ra.at[j], rs_r.at[0, j])
        part[j, right, upper, :] = (
            part[j, right, upper, :].astype(F32) + ra[j].astype(F32)
        ).astype(BF16)
        tp_copy(
            part.at[j, right, upper], fl.at[j, upper], rs_s.at[4, j], rs_r.at[4, j], right
        ).start()
        got(rb.at[j], rs_r.at[1, j])
        part[j, left, lower, :] = (
            part[j, left, lower, :].astype(F32) + rb[j].astype(F32)
        ).astype(BF16)
        tp_copy(
            part.at[j, left, lower], fr.at[j, lower], rs_s.at[5, j], rs_r.at[5, j], left
        ).start()

    def give_back(j):
        got(fl.at[j, lower], rs_r.at[2, j])
        got(fr.at[j, upper], rs_r.at[3, j])
        got(fl.at[j, upper], rs_r.at[4, j])
        got(fr.at[j, lower], rs_r.at[5, j])
        ret[j] = (part[j, tp].astype(F32) + fl[j].astype(F32) + fr[j].astype(F32)).astype(BF16)
        if j == 0:
            ret_in[0, pl.ds(mine, cap), :] = ret[0, pl.ds(mine, cap), :]
        exchange(
            ret,
            lambda j, at: ret_in.at[j, pl.ds(at, cap)],
            ret_s,
            ret_r,
            j,
            lax.rem(xpos + NX - j, NX),
        )

    own(0)
    own(1)
    forward(0)
    own(2)
    forward(1)
    for i in range(11, 14):
        loads[i].wait()
    experts(0)
    own(3)
    forward(2)
    add_on(0)
    experts(1)
    forward(3)
    give_back(0)
    add_on(1)
    experts(2)
    give_back(1)
    add_on(2)
    experts(3)
    give_back(2)
    add_on(3)
    give_back(3)

    lane = lax.broadcasted_iota(jnp.int32, (tokens, group), 1)
    spread = (lane // pair) * (NX * pair) + lax.rem(lane, pair)
    for j in range(NX):
        got(ret_in.at[j, pl.ds(0, rows_of(j))], ret_r.at[j])
        slot = (spread + lax.rem(xpos + j, NX) * pair).astype(F32)
        routed = hid[...]
        for k in range(2):
            pick = (slot == cols8[:, 1 + k : 2 + k]).astype(F32).astype(BF16)
            routed = routed + cols8[:, 3 + k : 4 + k] * jnp.dot(
                pick, ret_in[j], preferred_element_type=F32
            )
        hid[...] = routed
    out_ref[...] = hid[...].astype(BF16)

    for j in range(NX):
        got(outgo.at[j, pl.ds(0, rows_of(j))], disp_s.at[j])
        got(ret.at[j, pl.ds(0, rows_of(j))], ret_s.at[j])
        for i in range(2):
            got(xin.at[tp, j], ag_s.at[i, j])
        for i in range(2, 4):
            got(xin.at[tp, j, upper], ag_s.at[i, j])
        for i in range(6):
            got(part.at[j, 0, upper], rs_s.at[i, j])


def per_device(
    residual_in,
    conv_input,
    outer_gate,
    inner_gate,
    documents,
    conv_taps,
    mixer_gain,
    output_weight,
    ffn_gain,
    routes,
    route_weights,
    expert_gate,
    expert_up,
    expert_down,
):
    nsp = lax.axis_size("sp")
    ntp = lax.axis_size("tp")
    tokens, features = residual_in.shape
    channels = conv_input.shape[1]
    cap = 4 * tokens // nsp
    group = nsp // NX * cap
    half = group // 2
    width = features * ntp
    hidden_units = expert_gate.shape[2]
    args = (
        residual_in,
        conv_input,
        outer_gate,
        inner_gate,
        documents.reshape(1, tokens),
        conv_taps,
        mixer_gain.reshape(1, -1),
        output_weight,
        ffn_gain.reshape(1, -1),
        routes.T,
        route_weights.T,
        expert_gate,
        expert_up,
        expert_down,
    )
    locals_ = [
        pltpu.VMEM(a.shape if a.ndim == 2 else a.shape[1:], a.dtype) for a in args
    ]
    dma = pltpu.SemaphoreType.DMA
    scratch = locals_ + [
        pltpu.VMEM((8, tokens), F32),
        pltpu.VMEM((tokens, 8), F32),
        pltpu.VMEM((tokens + 8, channels), F32),
        pltpu.VMEM((tokens + 8, channels), F32),
        pltpu.VMEM((16, channels), F32),
        pltpu.VMEM((16, channels), F32),
        pltpu.VMEM((ntp, tokens, channels), BF16),
        pltpu.VMEM((ntp, 8, tokens), F32),
        pltpu.VMEM((tokens, features), F32),
        pltpu.VMEM((NX, group, tokens), BF16),
        pltpu.VMEM((NX, group, features), BF16),
        pltpu.VMEM((ntp, NX, group, features), BF16),
        pltpu.VMEM((group, hidden_units), BF16),
        pltpu.VMEM((NX, ntp, group, features), BF16),
        pltpu.VMEM((NX, half, features), BF16),
        pltpu.VMEM((NX, half, features), BF16),
        pltpu.VMEM((NX, group, features), BF16),
        pltpu.VMEM((NX, group, features), BF16),
        pltpu.VMEM((NX, group, features), BF16),
        pltpu.VMEM((NX, group, features), BF16),
        dma((len(args),)),
        dma((2,)),
        dma((ntp - 1,)),
        dma((ntp - 1,)),
        dma((ntp - 1,)),
        dma((ntp - 1,)),
        dma((NX,)),
        dma((NX,)),
        dma((4, NX)),
        dma((4, NX)),
        dma((6, NX)),
        dma((6, NX)),
        dma((NX,)),
        dma((NX,)),
    ]
    return pl.pallas_call(
        functools.partial(layer_kernel, nsp, ntp, cap),
        out_shape=jax.ShapeDtypeStruct((tokens, features), BF16),
        in_specs=[pl.BlockSpec(memory_space=pl.ANY)] * len(args),
        out_specs=pl.BlockSpec(memory_space=pltpu.VMEM),
        scratch_shapes=scratch,
        compiler_params=pltpu.CompilerParams(
            collective_id=0, has_side_effects=True, vmem_limit_bytes=60 * 1024 * 1024
        ),
        cost_estimate=pl.CostEstimate(
            flops=6 * nsp * cap * width * hidden_units,
            bytes_accessed=6 * width * hidden_units,
            transcendentals=0,
        ),
        name="layer",
    )(*args)


def solution(mesh):
    placed = (
        P("sp", "tp"),
        P("sp", "tp"),
        P("sp", "tp"),
        P("sp", "tp"),
        P("sp"),
        P(None, "tp"),
        P(),
        P(None, "tp"),
        P("tp"),
        P("sp", None),
        P("sp", None),
        P("sp", None, "tp"),
        P("sp", None, "tp"),
        P("sp", "tp", None),
    )
    return jax.shard_map(
        per_device, mesh=mesh, in_specs=placed, out_specs=P("sp", "tp"), check_vma=False
    )
```

```python
import functools

import jax
import jax.numpy as jnp
from jax import lax
from jax.experimental import pallas as pl
from jax.experimental.pallas import tpu as pltpu
from jax.sharding import PartitionSpec as P

EPS = 1e-06
CORES = 2
NX = 4
OFFSETS = (0, 1, -1, 2, -2, 3, -3, 4)
NEAR = 3
PIECES = ((3, 2), (5, 2), (7, 1), (1, 2), (0, 1))
ORDER = (
    ("tokens", 0),
    ("own", 0),
    ("near", 0),
    ("forward", 0),
    ("weights", 0),
    ("own", 1),
    ("up", 0),
    ("forward", 1),
    ("down", 0),
    ("own", 2),
    ("start", 0),
    ("upz", 0),
    ("downz", 0),
    ("up", 1),
    ("forward", 2),
    ("down", 1),
    ("add", 0),
    ("start", 1),
    ("up", 2),
    ("down", 2),
    ("start", 2),
    ("back", 0),
    ("upn", 0),
    ("add", 1),
    ("downn", 0),
    ("add", 2),
    ("start", 3),
    ("start", 4),
    ("back", 1),
    ("back", 2),
    ("add", 3),
    ("add", 4),
    ("combine", 0),
    ("back", 3),
    ("back", 4),
    ("combine", 1),
    ("combine", 2),
    ("gone", 0),
    ("combine", 4),
    ("combine", 3),
)
MESH = pl.DeviceIdType.MESH
F32 = jnp.float32
BF16 = jnp.bfloat16


def layer_kernel(
    nsp,
    ntp,
    cap,
    res_h,
    ci_h,
    og_h,
    ig_h,
    doc_h,
    taps_h,
    mg_h,
    ow_h,
    fg_h,
    rt_h,
    rw_h,
    wg_h,
    wu_h,
    wd_h,
    out_ref,
    res,
    ci,
    og,
    ig,
    doc,
    taps,
    mg,
    ow,
    fg,
    rt,
    rw,
    wg,
    wu,
    wd,
    rows8,
    cols8,
    joined,
    docj,
    halo_out,
    halo_in,
    gains,
    mix,
    tok,
    hid,
    perm,
    outgo,
    outrow,
    xin,
    scl,
    act,
    part,
    rx,
    fl,
    fr,
    ret,
    ret_in,
    load_sem,
    halo_sem,
    gain_s,
    gain_r,
    mix_s,
    mix_r,
    disp_s,
    disp_r,
    ag_s,
    ag_r,
    rs_s,
    rs_r,
    ret_s,
    ret_r,
    round_sem,
):
    sp = lax.axis_index("sp")
    tp = lax.axis_index("tp")
    nz = nsp // (NX * CORES)
    zpos = sp // (NX * CORES)
    xpos = (sp // CORES) % NX
    cpos = sp % CORES
    tokens, features = res.shape
    channels = ci.shape[1]
    peers = NX * CORES
    region = peers * cap
    left = lax.rem(tp + ntp - 1, ntp)
    right = lax.rem(tp + 1, ntp)
    opposite = lax.rem(tp + 2, ntp)

    def at_sp(dz, dx, core):
        return (
            lax.rem(zpos + (dz + nz), nz) * NX + lax.rem(xpos + dx, NX)
        ) * CORES + core

    def signal(sem, to):
        pl.semaphore_signal(sem, inc=1, device_id=to, device_id_type=MESH)

    barrier = pltpu.get_barrier_semaphore()
    for d in range(1, ntp):
        signal(barrier, (sp, lax.rem(tp + d, ntp)))
    for d in (1, nsp - 1):
        signal(barrier, (lax.rem(sp + d, nsp), tp))
    for d in range(1, NX):
        signal(barrier, (at_sp(0, d, cpos), tp))
    for d in (1, -1, 2, -2):
        signal(barrier, (at_sp(d, 0, cpos), tp))
    signal(barrier, (at_sp(0, 0, 1 - cpos), tp))
    greeted = ntp - 1 + 2 + NX - 1 + 4 + 1

    pairs = (
        (rt_h, rt),
        (doc_h, doc),
        (rw_h, rw),
        (ci_h, ci),
        (ig_h, ig),
        (og_h, og),
        (taps_h, taps),
        (fg_h, gains.at[tp]),
        (mg_h, mg),
        (ow_h, ow),
        (res_h, res),
        (wg_h.at[0], wg),
        (wu_h.at[0], wu),
        (wd_h.at[0], wd),
    )
    loads = [
        pltpu.make_async_copy(src, dst, load_sem.at[i]) for i, (src, dst) in enumerate(pairs)
    ]
    for load in loads:
        load.start()

    for i in range(3):
        loads[i].wait()
    experts_iota = lax.broadcasted_iota(jnp.int32, (nsp, tokens), 0)
    first = (experts_iota == rt[0:1, :]).astype(F32)
    second = (experts_iota == rt[1:2, :]).astype(F32)
    named = (first + second).astype(BF16)
    before = (
        lax.broadcasted_iota(jnp.int32, (tokens, tokens), 0)
        < lax.broadcasted_iota(jnp.int32, (tokens, tokens), 1)
    ).astype(F32).astype(BF16)
    earlier = jnp.dot(named, before, preferred_element_type=F32)
    slots = earlier + (experts_iota * cap).astype(F32)
    rows8[0:1, :] = doc[...].astype(F32)
    rows8[1:2, :] = jnp.sum(first * slots, axis=0, keepdims=True)
    rows8[2:3, :] = jnp.sum(second * slots, axis=0, keepdims=True)
    rows8[3:5, :] = rw[...]
    rows8[5:8, :] = jnp.zeros((3, tokens), F32)
    cols8[...] = jnp.transpose(rows8[...])

    for i in range(3, 8):
        loads[i].wait()
    value = (ig[...].astype(F32) * ci[...].astype(F32)).astype(BF16).astype(F32)
    joined[8:, :] = value
    docj[8:, :] = jnp.broadcast_to(cols8[:, 0:1], (tokens, channels))
    halo_out[0:8, :] = value[tokens - 8 :, :]
    halo_out[8:16, :] = jnp.broadcast_to(cols8[tokens - 8 :, 0:1], (8, channels))

    def convolve(lo, hi):
        docs_now = docj[8 + lo : 8 + hi, :]
        same_one = (docj[7 + lo : 7 + hi, :] == docs_now).astype(F32)
        same_two = (docj[6 + lo : 6 + hi, :] == docs_now).astype(F32)
        conv_sum = (
            taps[2:3, :] * joined[8 + lo : 8 + hi, :]
            + taps[1:2, :] * joined[7 + lo : 7 + hi, :] * same_one
            + taps[0:1, :] * joined[6 + lo : 6 + hi, :] * same_two
        )
        mix[tp, lo:hi, :] = (og[lo:hi, :].astype(F32) * conv_sum).astype(BF16)

    def to_tp(ref, send, recv):
        copies = []
        for d in (2, 1, ntp - 1):
            copies.append(
                pltpu.make_async_remote_copy(
                    src_ref=ref,
                    dst_ref=ref,
                    send_sem=send.at[d - 1],
                    recv_sem=recv.at[d - 1],
                    device_id=(sp, lax.rem(tp + d, ntp)),
                    device_id_type=MESH,
                )
            )
        for copy in copies:
            copy.start()
        return copies

    edge = 16
    convolve(edge, tokens)
    with jax.named_scope("barrier"):
        pl.semaphore_wait(barrier, greeted)
    halo = pltpu.make_async_remote_copy(
        src_ref=halo_out,
        dst_ref=halo_in,
        send_sem=halo_sem.at[0],
        recv_sem=halo_sem.at[1],
        device_id=(lax.rem(sp + 1, nsp), tp),
        device_id_type=MESH,
    )
    halo.start()
    for d in (2, -2):
        signal(round_sem.at[0], (at_sp(d, 0, cpos), tp))
    copies = to_tp(mix.at[tp, pl.ds(edge, tokens - edge)], mix_s.at[0], mix_r.at[0])
    copies += to_tp(gains.at[tp], gain_s, gain_r)

    line = lax.broadcasted_iota(jnp.int32, (region, tokens), 0)
    for r, dz in enumerate(OFFSETS):
        slot = (line + lax.rem(zpos + (dz + nz), nz) * region).astype(F32)
        hit = (slot == rows8[1:2, :]) | (slot == rows8[2:3, :])
        perm[r] = hit.astype(F32).astype(BF16)

    with jax.named_scope("halowait"):
        halo.wait()
    joined[0:8, :] = halo_in[0:8, :]
    docj[0:8, :] = jnp.where(sp == 0, -1.0, halo_in[8:16, :])
    convolve(0, edge)
    copies += to_tp(mix.at[tp, pl.ds(0, edge)], mix_s.at[1], mix_r.at[1])
    pl.semaphore_wait(round_sem.at[0], 2)
    for d in range(1, NX):
        signal(round_sem.at[1], (at_sp(0, d, cpos), tp))

    for i in range(8, 11):
        loads[i].wait()
    with jax.named_scope("mixwait"):
        for copy in copies:
            copy.wait()
    pl.semaphore_wait(round_sem.at[1], NX - 1)
    signal(round_sem.at[2], (at_sp(0, 0, 1 - cpos), tp))
    pieces = jnp.concatenate([mix[q] for q in range(ntp)], axis=1).astype(F32)
    squares = jnp.sum(pieces * pieces, axis=1, keepdims=True)
    mix_scale = lax.rsqrt(squares / (channels * ntp) + EPS)
    scaled = (pieces * mg[...]).astype(BF16)
    projected = jnp.dot(scaled, ow[...], preferred_element_type=F32)
    hidden = res[...].astype(F32) + projected * mix_scale
    hid[...] = hidden
    gained = (hidden * gains[tp]).astype(BF16)
    tok[tp] = gained

    def tp_copy(src, dst, send, recv, to):
        return pltpu.make_async_remote_copy(
            src_ref=src,
            dst_ref=dst,
            send_sem=send,
            recv_sem=recv,
            device_id=(sp, to),
            device_id_type=MESH,
        )

    def got(ref, sem):
        with jax.named_scope("wait"):
            pltpu.make_async_copy(ref, ref, sem).wait()

    def ring_own(buffer, start, rows, k):
        half = rows // 2
        upper = buffer.at[tp, pl.ds(start, half)]
        lower = buffer.at[tp, pl.ds(start + half, half)]
        tp_copy(upper, upper, ag_s.at[0, k], ag_r.at[0, k], right).start()
        tp_copy(lower, lower, ag_s.at[1, k], ag_r.at[1, k], left).start()
        tp_copy(lower, lower, ag_s.at[2, k], ag_r.at[2, k], right).start()
        tp_copy(upper, upper, ag_s.at[3, k], ag_r.at[3, k], left).start()

    def ring_forward(buffer, start, rows, k):
        half = rows // 2
        upper = buffer.at[left, pl.ds(start, half)]
        lower = buffer.at[right, pl.ds(start + half, half)]
        got(upper, ag_r.at[0, k])
        tp_copy(upper, upper, ag_s.at[4, k], ag_r.at[4, k], right).start()
        got(lower, ag_r.at[1, k])
        tp_copy(lower, lower, ag_s.at[5, k], ag_r.at[5, k], left).start()

    def ring_rest(buffer, start, rows, k):
        half = rows // 2
        got(buffer.at[left, pl.ds(start + half, half)], ag_r.at[2, k])
        got(buffer.at[right, pl.ds(start, half)], ag_r.at[3, k])
        got(buffer.at[opposite, pl.ds(start, half)], ag_r.at[4, k])
        got(buffer.at[opposite, pl.ds(start + half, half)], ag_r.at[5, k])

    tokens_piece = len(PIECES)
    ring_own(tok, 0, tokens, tokens_piece)
    with jax.named_scope("roundwait"):
        pl.semaphore_wait(round_sem.at[2], 1)

    mine = xpos * CORES + cpos
    my_rows = pl.multiple_of(mine * cap, cap)

    def exchange(src, dst, send, recv, r, dz):
        zz = lax.rem(zpos + (dz + nz), nz)

        def one(i, carry):
            to = lax.rem(mine + i, peers)
            pltpu.make_async_remote_copy(
                src_ref=src(r, pl.multiple_of(to * cap, cap)),
                dst_ref=dst(r, my_rows),
                send_sem=send.at[r],
                recv_sem=recv.at[r],
                device_id=(zz * peers + to, tp),
                device_id_type=MESH,
            ).start()
            return carry

        lax.fori_loop(1 if r == 0 else 0, peers, one, 0)

    def rows_of(r):
        return region - cap if r == 0 else region

    for r in range(NEAR, len(OFFSETS)):
        outgo[r - NEAR] = jnp.dot(perm[r], gained, preferred_element_type=F32).astype(BF16)
        exchange(
            lambda r, at: outgo.at[r - NEAR, pl.ds(at, cap)],
            lambda r, at: xin.at[tp, pl.ds(r * region + at, cap)],
            disp_s,
            disp_r,
            r,
            OFFSETS[r],
        )

    def near():
        ring_rest(tok, 0, tokens, tokens_piece)
        for r in range(NEAR):
            for q in range(ntp):
                outrow[q, r * region : (r + 1) * region, :] = jnp.dot(
                    perm[r], tok[q], preferred_element_type=F32
                ).astype(BF16)
            if r == 0:
                for q in range(ntp):
                    xin[q, pl.ds(my_rows, cap), :] = outrow[q, pl.ds(my_rows, cap), :]
            exchange(
                lambda r, at: outrow.at[:, pl.ds(r * region + at, cap)],
                lambda r, at: xin.at[:, pl.ds(r * region + at, cap)],
                disp_s,
                disp_r,
                r,
                OFFSETS[r],
            )

    def arrived(k):
        first_region, count = PIECES[k]
        for r in range(first_region, first_region + count):
            if r < NEAR:
                got(xin.at[:, pl.ds(r * region, rows_of(r))], disp_r.at[r])
            else:
                got(xin.at[tp, pl.ds(r * region, region)], disp_r.at[r])

    def span(k):
        return PIECES[k][0] * region, PIECES[k][1] * region

    def own(k):
        arrived(k)
        ring_own(xin, *span(k), k)

    def forward(k):
        ring_forward(xin, *span(k), k)

    width = features * ntp
    hidden_units = wg.shape[1]
    tile = 128
    wide = 256

    def experts_up(start, rows):
        total = jnp.zeros((rows, tile), F32)
        for q in range(ntp):
            weight = 1.0 / (gains[q] * gains[q])
            for c in range(features // tile):
                cut = slice(c * tile, (c + 1) * tile)
                x = xin[q, start : start + rows, cut].astype(F32)
                total = total + x * x * weight[:, cut]
        scale = lax.rsqrt(jnp.sum(total, axis=1, keepdims=True) / width + EPS)
        scl[0:rows, :] = jnp.broadcast_to(scale, (rows, tile))

        def up_tile(n, carry):
            at = pl.ds(pl.multiple_of(n * tile, tile), tile)
            x = jnp.concatenate([xin[q, start : start + rows] for q in range(ntp)], axis=1)
            both = jnp.concatenate([wg[:, at], wu[:, at]], axis=1)
            made = jnp.dot(x, both, preferred_element_type=F32)
            gate = made[:, :tile] * scl[0:rows, :]
            act[0:rows, at] = (
                jax.nn.silu(gate) * (made[:, tile:] * scl[0:rows, :])
            ).astype(BF16)
            return carry

        lax.fori_loop(0, hidden_units // tile, up_tile, 0)

    def experts_down(start, rows):
        for q in range(ntp):
            for k in range(features // wide):
                cols = slice(q * features + k * wide, q * features + (k + 1) * wide)
                part[q, start : start + rows, k * wide : (k + 1) * wide] = jnp.dot(
                    act[0:rows, :], wd[:, cols], preferred_element_type=F32
                ).astype(BF16)

    def reduce_start(k):
        start, rows = span(k)
        half = rows // 2
        upper = pl.ds(start, half)
        lower = pl.ds(start + half, half)
        tp_copy(part.at[opposite, upper], rx.at[upper], rs_s.at[0, k], rs_r.at[0, k], right).start()
        tp_copy(part.at[opposite, lower], rx.at[lower], rs_s.at[1, k], rs_r.at[1, k], left).start()
        tp_copy(part.at[right, lower], fl.at[lower], rs_s.at[2, k], rs_r.at[2, k], right).start()
        tp_copy(part.at[left, upper], fr.at[upper], rs_s.at[3, k], rs_r.at[3, k], left).start()

    def reduce_add(k):
        start, rows = span(k)
        half = rows // 2
        upper = pl.ds(start, half)
        lower = pl.ds(start + half, half)
        got(rx.at[upper], rs_r.at[0, k])
        part[right, upper, :] = (
            part[right, upper, :].astype(F32) + rx[upper, :].astype(F32)
        ).astype(BF16)
        tp_copy(part.at[right, upper], fl.at[upper], rs_s.at[4, k], rs_r.at[4, k], right).start()
        got(rx.at[lower], rs_r.at[1, k])
        part[left, lower, :] = (
            part[left, lower, :].astype(F32) + rx[lower, :].astype(F32)
        ).astype(BF16)
        tp_copy(part.at[left, lower], fr.at[lower], rs_s.at[5, k], rs_r.at[5, k], left).start()

    def give_back(k):
        start, rows = span(k)
        half = rows // 2
        upper = pl.ds(start, half)
        lower = pl.ds(start + half, half)
        got(fl.at[lower], rs_r.at[2, k])
        got(fr.at[upper], rs_r.at[3, k])
        got(fl.at[upper], rs_r.at[4, k])
        got(fr.at[lower], rs_r.at[5, k])
        whole = pl.ds(start, rows)
        ret[whole, :] = (
            part[tp, whole, :].astype(F32) + fl[whole, :].astype(F32) + fr[whole, :].astype(F32)
        ).astype(BF16)
        first_region, count = PIECES[k]
        for r in range(first_region, first_region + count):
            if r == 0:
                ret_in[pl.ds(my_rows, cap), :] = ret[pl.ds(my_rows, cap), :]
            exchange(
                lambda r, at: ret.at[pl.ds(r * region + at, cap)],
                lambda r, at: ret_in.at[pl.ds(r * region + at, cap)],
                ret_s,
                ret_r,
                r,
                -OFFSETS[r],
            )

    lane = lax.broadcasted_iota(jnp.int32, (tokens, region), 1)

    def combine(k):
        first_region, count = PIECES[k]
        for r in range(first_region, first_region + count):
            got(ret_in.at[pl.ds(r * region, rows_of(r))], ret_r.at[r])
        start, rows = span(k)
        picks = [[], []]
        for r in range(first_region, first_region + count):
            slot = (lane + lax.rem(zpos + (OFFSETS[r] + nz), nz) * region).astype(F32)
            for i in range(2):
                picks[i].append((slot == cols8[:, 1 + i : 2 + i]).astype(F32).astype(BF16))
        routed = hid[...]
        for i in range(2):
            pick = jnp.concatenate(picks[i], axis=1)
            routed = routed + cols8[:, 3 + i : 4 + i] * jnp.dot(
                pick, ret_in[start : start + rows, :], preferred_element_type=F32
            )
        hid[...] = routed

    def gone(ref, sem):
        pltpu.make_async_copy(ref, ref, sem).wait()

    def all_gone():
        for r in range(len(OFFSETS)):
            if r < NEAR:
                gone(outrow.at[:, pl.ds(0, rows_of(r))], disp_s.at[r])
            else:
                gone(outgo.at[r - NEAR], disp_s.at[r])
            gone(ret.at[pl.ds(0, rows_of(r))], ret_s.at[r])
        for k in range(len(PIECES)):
            half = span(k)[1] // 2
            for i in range(6):
                if k < 3:
                    gone(xin.at[tp, pl.ds(0, half)], ag_s.at[i, k])
                gone(part.at[0, pl.ds(0, half)], rs_s.at[i, k])
        for i in range(6):
            gone(tok.at[tp, pl.ds(0, tokens // 2)], ag_s.at[i, tokens_piece])

    steps = {
        "own": own,
        "forward": forward,
        "up": lambda k: (ring_rest(xin, *span(k), k), experts_up(*span(k))),
        "down": lambda k: experts_down(*span(k)),
        "add": reduce_add,
        "back": give_back,
        "combine": combine,
        "tokens": lambda k: ring_forward(tok, 0, tokens, tokens_piece),
        "near": lambda k: near(),
        "weights": lambda k: [loads[i].wait() for i in range(11, 14)],
        "upz": lambda k: (arrived(4), experts_up(*span(4))),
        "downz": lambda k: experts_down(*span(4)),
        "upn": lambda k: (arrived(3), experts_up(*span(3))),
        "downn": lambda k: experts_down(*span(3)),
        "start": reduce_start,
        "gone": lambda k: all_gone(),
    }
    for name, k in ORDER:
        with jax.named_scope(f"{name}{k}"):
            steps[name](k)
    with jax.named_scope("out"):
        out_ref[...] = hid[...].astype(BF16)

def per_device(
    residual_in,
    conv_input,
    outer_gate,
    inner_gate,
    documents,
    conv_taps,
    mixer_gain,
    output_weight,
    ffn_gain,
    routes,
    route_weights,
    expert_gate,
    expert_up,
    expert_down,
):
    nsp = lax.axis_size("sp")
    ntp = lax.axis_size("tp")
    tokens, features = residual_in.shape
    channels = conv_input.shape[1]
    cap = 4 * tokens // nsp
    region = NX * CORES * cap
    slots = nsp * cap
    width = features * ntp
    hidden_units = expert_gate.shape[2]
    args = (
        residual_in,
        conv_input,
        outer_gate,
        inner_gate,
        documents.reshape(1, tokens),
        conv_taps,
        mixer_gain.reshape(1, -1),
        output_weight,
        ffn_gain.reshape(1, -1),
        routes.T,
        route_weights.T,
        expert_gate,
        expert_up,
        expert_down,
    )
    locals_ = [
        pltpu.VMEM(a.shape if a.ndim == 2 else a.shape[1:], a.dtype) for a in args
    ]
    dma = pltpu.SemaphoreType.DMA
    scratch = locals_ + [
        pltpu.VMEM((8, tokens), F32),
        pltpu.VMEM((tokens, 8), F32),
        pltpu.VMEM((tokens + 8, channels), F32),
        pltpu.VMEM((tokens + 8, channels), F32),
        pltpu.VMEM((16, channels), F32),
        pltpu.VMEM((16, channels), F32),
        pltpu.VMEM((ntp, 1, features), F32),
        pltpu.VMEM((ntp, tokens, channels), BF16),
        pltpu.VMEM((ntp, tokens, features), BF16),
        pltpu.VMEM((tokens, features), F32),
        pltpu.VMEM((len(OFFSETS), region, tokens), BF16),
        pltpu.VMEM((len(OFFSETS) - NEAR, region, features), BF16),
        pltpu.VMEM((ntp, NEAR * region, features), BF16),
        pltpu.VMEM((ntp, slots, features), BF16),
        pltpu.VMEM((NEAR * region, 128), F32),
        pltpu.VMEM((NEAR * region, hidden_units), BF16),
        pltpu.VMEM((ntp, slots, features), BF16),
        pltpu.VMEM((slots, features), BF16),
        pltpu.VMEM((slots, features), BF16),
        pltpu.VMEM((slots, features), BF16),
        pltpu.VMEM((slots, features), BF16),
        pltpu.VMEM((slots, features), BF16),
        dma((len(args),)),
        dma((2,)),
        dma((ntp - 1,)),
        dma((ntp - 1,)),
        dma((2, ntp - 1)),
        dma((2, ntp - 1)),
        dma((len(OFFSETS),)),
        dma((len(OFFSETS),)),
        dma((6, len(PIECES) + 1)),
        dma((6, len(PIECES) + 1)),
        dma((6, len(PIECES))),
        dma((6, len(PIECES))),
        dma((len(OFFSETS),)),
        dma((len(OFFSETS),)),
        pltpu.SemaphoreType.REGULAR((3,)),
    ]
    return pl.pallas_call(
        functools.partial(layer_kernel, nsp, ntp, cap),
        out_shape=jax.ShapeDtypeStruct((tokens, features), BF16),
        in_specs=[pl.BlockSpec(memory_space=pl.ANY)] * len(args),
        out_specs=pl.BlockSpec(memory_space=pltpu.VMEM),
        scratch_shapes=scratch,
        compiler_params=pltpu.CompilerParams(
            collective_id=0, has_side_effects=True, vmem_limit_bytes=60 * 1024 * 1024
        ),
        cost_estimate=pl.CostEstimate(
            flops=6 * nsp * cap * width * hidden_units,
            bytes_accessed=6 * width * hidden_units,
            transcendentals=0,
        ),
        name="layer",
    )(*args)


def solution(mesh):
    placed = (
        P("sp", "tp"),
        P("sp", "tp"),
        P("sp", "tp"),
        P("sp", "tp"),
        P("sp"),
        P(None, "tp"),
        P(),
        P(None, "tp"),
        P("tp"),
        P("sp", None),
        P("sp", None),
        P("sp", None, "tp"),
        P("sp", None, "tp"),
        P("sp", "tp", None),
    )
    return jax.shard_map(
        per_device, mesh=mesh, in_specs=placed, out_specs=P("sp", "tp"), check_vma=False
    )
```

```python
import functools

import jax
import jax.numpy as jnp
from jax import lax
from jax.experimental import pallas as pl
from jax.experimental.pallas import tpu as pltpu
from jax.sharding import PartitionSpec as P

EPS = 1e-06
CORES = 2
NX = 4
REGIONS = (
    (0, 0, 8),
    (1, 0, 8),
    (-1, 0, 8),
    (2, 0, 4),
    (-2, 0, 4),
    (2, 4, 4),
    (-2, 4, 4),
    (3, 0, 4),
    (-3, 0, 4),
    (3, 4, 4),
    (-3, 4, 4),
    (4, 0, 8),
)
NEAR = 3
RINGS = ((3, 4), (5, 6), (7, 8), (9, 10), (11,))
RING = len(RINGS)
PIECES = ((3, 4, 5, 6), (7, 8, 9, 10), (11,), (1, 2), (0,))
ORDER = (
    ("tokens", 0),
    ("own", 0),
    ("near", 0),
    ("own", 1),
    ("forward", 0),
    ("own", 2),
    ("forward", 1),
    ("forward", 2),
    ("own", 3),
    ("weights", 0),
    ("rest", 0),
    ("rest", 1),
    ("up", 0),
    ("forward", 3),
    ("down", 0),
    ("own", 4),
    ("start", 0),
    ("up", 4),
    ("down", 4),
    ("rest", 2),
    ("rest", 3),
    ("up", 1),
    ("forward", 4),
    ("down", 1),
    ("add", 0),
    ("start", 1),
    ("up", 3),
    ("down", 3),
    ("back", 0),
    ("rest", 4),
    ("up", 2),
    ("add", 1),
    ("down", 2),
    ("start", 2),
    ("start", 4),
    ("back", 1),
    ("add", 2),
    ("start", 3),
    ("add", 4),
    ("back", 2),
    ("combine", 0),
    ("add", 3),
    ("back", 4),
    ("back", 3),
    ("combine", 1),
    ("combine", 2),
    ("gone", 0),
    ("combine", 4),
    ("combine", 3),
)
MESH = pl.DeviceIdType.MESH
F32 = jnp.float32
BF16 = jnp.bfloat16


def layer_kernel(
    nsp,
    ntp,
    cap,
    res_h,
    ci_h,
    og_h,
    ig_h,
    doc_h,
    taps_h,
    mg_h,
    ow_h,
    fg_h,
    rt_h,
    rw_h,
    wg_h,
    wu_h,
    wd_h,
    out_ref,
    res,
    ci,
    og,
    ig,
    doc,
    taps,
    mg,
    ow,
    fg,
    rt,
    rw,
    wg,
    wu,
    wd,
    rows8,
    cols8,
    joined,
    docj,
    halo_out,
    halo_in,
    gains,
    mix,
    tok,
    hid,
    perm,
    outgo,
    outrow,
    xin,
    scl,
    act,
    part,
    rx,
    fl,
    fr,
    ret,
    ret_in,
    load_sem,
    halo_sem,
    mix_s,
    mix_r,
    disp_s,
    disp_r,
    ag_s,
    ag_r,
    rs_s,
    rs_r,
    ret_s,
    ret_r,
    round_sem,
):
    sp = lax.axis_index("sp")
    tp = lax.axis_index("tp")
    nz = nsp // (NX * CORES)
    zpos = sp // (NX * CORES)
    xpos = (sp // CORES) % NX
    cpos = sp % CORES
    tokens, features = res.shape
    channels = ci.shape[1]
    peers = NX * CORES
    plane = peers * cap
    mine = xpos * CORES + cpos
    base, most = [], 0
    for _, _, count in REGIONS:
        base.append(most)
        most += count * cap
    sizes = [count * cap for _, _, count in REGIONS]
    left = lax.rem(tp + ntp - 1, ntp)
    right = lax.rem(tp + 1, ntp)
    opposite = lax.rem(tp + 2, ntp)

    def at_sp(dz, dx, core):
        return (
            lax.rem(zpos + (dz + nz), nz) * NX + lax.rem(xpos + dx, NX)
        ) * CORES + core

    def signal(sem, to):
        pl.semaphore_signal(sem, inc=1, device_id=to, device_id_type=MESH)

    barrier = pltpu.get_barrier_semaphore()
    for d in range(1, ntp):
        signal(barrier, (sp, lax.rem(tp + d, ntp)))
    for d in (1, nsp - 1):
        signal(barrier, (lax.rem(sp + d, nsp), tp))
    for d in range(1, NX):
        signal(barrier, (at_sp(0, d, cpos), tp))
    for d in (1, -1, 2, -2):
        signal(barrier, (at_sp(d, 0, cpos), tp))
    signal(barrier, (at_sp(0, 0, 1 - cpos), tp))
    greeted = ntp - 1 + 2 + NX - 1 + 4 + 1

    pairs = (
        (rt_h, rt),
        (doc_h, doc),
        (rw_h, rw),
        (ci_h, ci),
        (ig_h, ig),
        (og_h, og),
        (taps_h, taps),
        (fg_h, gains.at[tp]),
        (mg_h, mg),
        (ow_h, ow),
        (res_h, res),
        (wg_h.at[0], wg),
        (wu_h.at[0], wu),
        (wd_h.at[0], wd),
    )
    loads = [
        pltpu.make_async_copy(src, dst, load_sem.at[i]) for i, (src, dst) in enumerate(pairs)
    ]
    for load in loads:
        load.start()

    for i in range(3):
        loads[i].wait()
    experts_iota = lax.broadcasted_iota(jnp.int32, (nsp, tokens), 0)
    first = (experts_iota == rt[0:1, :]).astype(F32)
    second = (experts_iota == rt[1:2, :]).astype(F32)
    named = (first + second).astype(BF16)
    before = (
        lax.broadcasted_iota(jnp.int32, (tokens, tokens), 0)
        < lax.broadcasted_iota(jnp.int32, (tokens, tokens), 1)
    ).astype(F32).astype(BF16)
    earlier = jnp.dot(named, before, preferred_element_type=F32)
    slots = earlier + (experts_iota * cap).astype(F32)
    rows8[0:1, :] = doc[...].astype(F32)
    rows8[1:2, :] = jnp.sum(first * slots, axis=0, keepdims=True)
    rows8[2:3, :] = jnp.sum(second * slots, axis=0, keepdims=True)
    rows8[3:5, :] = rw[...]
    rows8[5:8, :] = jnp.zeros((3, tokens), F32)
    cols8[...] = jnp.transpose(rows8[...])

    for i in range(3, 8):
        loads[i].wait()
    value = (ig[...].astype(F32) * ci[...].astype(F32)).astype(BF16).astype(F32)
    joined[8:, :] = value
    docj[8:, :] = jnp.broadcast_to(cols8[:, 0:1], (tokens, channels))
    halo_out[0:8, :] = value[tokens - 8 :, :]
    halo_out[8:16, :] = jnp.broadcast_to(cols8[tokens - 8 :, 0:1], (8, channels))

    def convolve(lo, hi):
        docs_now = docj[8 + lo : 8 + hi, :]
        same_one = (docj[7 + lo : 7 + hi, :] == docs_now).astype(F32)
        same_two = (docj[6 + lo : 6 + hi, :] == docs_now).astype(F32)
        conv_sum = (
            taps[2:3, :] * joined[8 + lo : 8 + hi, :]
            + taps[1:2, :] * joined[7 + lo : 7 + hi, :] * same_one
            + taps[0:1, :] * joined[6 + lo : 6 + hi, :] * same_two
        )
        mix[tp, lo:hi, :] = (og[lo:hi, :].astype(F32) * conv_sum).astype(BF16)

    def to_tp(ref, send, recv):
        for d in (2, 1, ntp - 1):
            pltpu.make_async_remote_copy(
                src_ref=ref,
                dst_ref=ref,
                send_sem=send,
                recv_sem=recv,
                device_id=(sp, lax.rem(tp + d, ntp)),
                device_id_type=MESH,
            ).start()

    def got(ref, sem):
        with jax.named_scope("wait"):
            pltpu.make_async_copy(ref, ref, sem).wait()

    edge = 16
    convolve(edge, tokens)
    with jax.named_scope("barrier"):
        pl.semaphore_wait(barrier, greeted)
    halo = pltpu.make_async_remote_copy(
        src_ref=halo_out,
        dst_ref=halo_in,
        send_sem=halo_sem.at[0],
        recv_sem=halo_sem.at[1],
        device_id=(lax.rem(sp + 1, nsp), tp),
        device_id_type=MESH,
    )
    halo.start()
    for d in (2, -2):
        signal(round_sem.at[0], (at_sp(d, 0, cpos), tp))
    to_tp(mix.at[tp, pl.ds(edge, tokens - edge)], mix_s.at[0], mix_r.at[0])
    to_tp(gains.at[tp], mix_s.at[1], mix_r.at[1])

    def slots_of(r, shape, dim):
        dz, skip, _ = REGIONS[r]
        line = lax.broadcasted_iota(jnp.int32, shape, dim)
        peer = lax.rem(line // cap + (mine + skip), peers)
        zz = lax.rem(zpos + (dz + nz), nz)
        return (zz * plane + peer * cap + lax.rem(line, cap)).astype(F32)

    for r in range(len(REGIONS)):
        slot = slots_of(r, (sizes[r], tokens), 0)
        hit = (slot == rows8[1:2, :]) | (slot == rows8[2:3, :])
        perm[base[r] : base[r] + sizes[r], :] = hit.astype(F32).astype(BF16)

    with jax.named_scope("halowait"):
        halo.wait()
    joined[0:8, :] = halo_in[0:8, :]
    docj[0:8, :] = jnp.where(sp == 0, -1.0, halo_in[8:16, :])
    convolve(0, edge)
    to_tp(mix.at[tp, pl.ds(0, edge)], mix_s.at[0], mix_r.at[0])
    pl.semaphore_wait(round_sem.at[0], 2)
    for d in range(1, NX):
        signal(round_sem.at[1], (at_sp(0, d, cpos), tp))

    for i in range(8, 11):
        loads[i].wait()
    with jax.named_scope("mixwait"):
        got(mix.at[pl.ds(0, ntp - 1)], mix_r.at[0])
        got(gains.at[pl.ds(0, ntp - 1)], mix_r.at[1])
    pl.semaphore_wait(round_sem.at[1], NX - 1)
    signal(round_sem.at[2], (at_sp(0, 0, 1 - cpos), tp))
    pieces = jnp.concatenate([mix[q] for q in range(ntp)], axis=1).astype(F32)
    squares = jnp.sum(pieces * pieces, axis=1, keepdims=True)
    mix_scale = lax.rsqrt(squares / (channels * ntp) + EPS)
    scaled = (pieces * mg[...]).astype(BF16)
    projected = jnp.dot(scaled, ow[...], preferred_element_type=F32)
    hidden = res[...].astype(F32) + projected * mix_scale
    hid[...] = hidden
    gained = (hidden * gains[tp]).astype(BF16)
    tok[tp] = gained

    def tp_copy(src, dst, send, recv, to):
        return pltpu.make_async_remote_copy(
            src_ref=src,
            dst_ref=dst,
            send_sem=send,
            recv_sem=recv,
            device_id=(sp, to),
            device_id_type=MESH,
        )

    def ring_own(buffer, start, rows, k):
        half = rows // 2
        upper = buffer.at[tp, pl.ds(start, half)]
        lower = buffer.at[tp, pl.ds(start + half, half)]
        tp_copy(upper, upper, ag_s.at[0], ag_r.at[0, k], right).start()
        tp_copy(lower, lower, ag_s.at[0], ag_r.at[1, k], left).start()
        tp_copy(lower, lower, ag_s.at[0], ag_r.at[2, k], right).start()
        tp_copy(upper, upper, ag_s.at[0], ag_r.at[2, k], left).start()

    def ring_forward(buffer, start, rows, k):
        half = rows // 2
        upper = buffer.at[left, pl.ds(start, half)]
        lower = buffer.at[right, pl.ds(start + half, half)]
        got(upper, ag_r.at[0, k])
        tp_copy(upper, upper, ag_s.at[0], ag_r.at[2, k], right).start()
        got(lower, ag_r.at[1, k])
        tp_copy(lower, lower, ag_s.at[0], ag_r.at[2, k], left).start()

    def ring_rest(buffer, start, rows, k):
        got(buffer.at[pl.ds(0, 2), pl.ds(start, rows)], ag_r.at[2, k])

    ring_own(tok, 0, tokens, RING)
    with jax.named_scope("roundwait"):
        pl.semaphore_wait(round_sem.at[2], 1)

    def exchange(src, dst, send, recv, r, way):
        dz, skip, count = REGIONS[r]
        zz = lax.rem(zpos + (way * dz + nz), nz)

        def one(i, carry):
            at = pl.ds(pl.multiple_of(base[r] + i * cap, cap), cap)
            to = lax.rem(mine + way * (i + skip) + peers, peers)
            pltpu.make_async_remote_copy(
                src_ref=src(at),
                dst_ref=dst(at),
                send_sem=send,
                recv_sem=recv,
                device_id=(zz * peers + to, tp),
                device_id_type=MESH,
            ).start()
            return carry

        lax.fori_loop(1 if r == 0 else 0, count, one, 0)

    ring_of = {r: g for g, regions in enumerate(RINGS) for r in regions}

    def extent(regions):
        return base[regions[0]], sum(sizes[r] for r in regions)

    def crossed(regions):
        start, rows = extent(regions)
        skip = cap if 0 in regions else 0
        return pl.ds(start + skip, rows - skip)

    def rows_at(r):
        return slice(base[r], base[r] + sizes[r])

    for r in range(NEAR, len(REGIONS)):
        outgo[rows_at(r), :] = jnp.dot(
            perm[rows_at(r), :], gained, preferred_element_type=F32
        ).astype(BF16)
        exchange(
            lambda at: outgo.at[at],
            lambda at: xin.at[tp, at],
            disp_s.at[0],
            disp_r.at[ring_of[r]],
            r,
            1,
        )

    def near():
        ring_rest(tok, 0, tokens, RING)
        for r in range(NEAR):
            for q in range(ntp):
                outrow[q, rows_at(r), :] = jnp.dot(
                    perm[rows_at(r), :], tok[q], preferred_element_type=F32
                ).astype(BF16)
            if r == 0:
                for q in range(ntp):
                    xin[q, 0:cap, :] = outrow[q, 0:cap, :]
            exchange(
                lambda at: outrow.at[:, at],
                lambda at: xin.at[:, at],
                disp_s.at[1],
                disp_r.at[RING + min(r, 1)],
                r,
                1,
            )

    def span(k):
        return extent(PIECES[k])

    def arrived(k):
        if PIECES[k][0] < NEAR:
            got(xin.at[:, crossed(PIECES[k])], disp_r.at[RING + min(PIECES[k][0], 1)])

    def own(g):
        got(xin.at[tp, crossed(RINGS[g])], disp_r.at[g])
        ring_own(xin, *extent(RINGS[g]), g)

    def forward(g):
        ring_forward(xin, *extent(RINGS[g]), g)

    def rest(g):
        ring_rest(xin, *extent(RINGS[g]), g)

    width = features * ntp
    hidden_units = wg.shape[1]
    tile = 128
    wide = 256

    def experts_up(start, rows):
        total = jnp.zeros((rows, tile), F32)
        for q in range(ntp):
            weight = 1.0 / (gains[q] * gains[q])
            for c in range(features // tile):
                cut = slice(c * tile, (c + 1) * tile)
                x = xin[q, start : start + rows, cut].astype(F32)
                total = total + x * x * weight[:, cut]
        scale = lax.rsqrt(jnp.sum(total, axis=1, keepdims=True) / width + EPS)
        scl[0:rows, :] = jnp.broadcast_to(scale, (rows, tile))

        def up_tile(n, carry):
            at = pl.ds(pl.multiple_of(n * tile, tile), tile)
            x = jnp.concatenate([xin[q, start : start + rows] for q in range(ntp)], axis=1)
            both = jnp.concatenate([wg[:, at], wu[:, at]], axis=1)
            made = jnp.dot(x, both, preferred_element_type=F32)
            gate = made[:, :tile] * scl[0:rows, :]
            act[0:rows, at] = (
                jax.nn.silu(gate) * (made[:, tile:] * scl[0:rows, :])
            ).astype(BF16)
            return carry

        lax.fori_loop(0, hidden_units // tile, up_tile, 0)

    def experts_down(start, rows):
        for q in range(ntp):
            for k in range(features // wide):
                cols = slice(q * features + k * wide, q * features + (k + 1) * wide)
                part[q, start : start + rows, k * wide : (k + 1) * wide] = jnp.dot(
                    act[0:rows, :], wd[:, cols], preferred_element_type=F32
                ).astype(BF16)

    def reduce_start(k):
        start, rows = span(k)
        half = rows // 2
        upper = pl.ds(start, half)
        lower = pl.ds(start + half, half)
        tp_copy(part.at[opposite, upper], rx.at[upper], rs_s.at[0], rs_r.at[0, k], right).start()
        tp_copy(part.at[opposite, lower], rx.at[lower], rs_s.at[0], rs_r.at[1, k], left).start()
        tp_copy(part.at[right, lower], fl.at[lower], rs_s.at[0], rs_r.at[2, k], right).start()
        tp_copy(part.at[left, upper], fr.at[upper], rs_s.at[0], rs_r.at[2, k], left).start()

    def reduce_add(k):
        start, rows = span(k)
        half = rows // 2
        upper = pl.ds(start, half)
        lower = pl.ds(start + half, half)
        got(rx.at[upper], rs_r.at[0, k])
        part[right, upper, :] = (
            part[right, upper, :].astype(F32) + rx[upper, :].astype(F32)
        ).astype(BF16)
        tp_copy(part.at[right, upper], fl.at[upper], rs_s.at[0], rs_r.at[2, k], right).start()
        got(rx.at[lower], rs_r.at[1, k])
        part[left, lower, :] = (
            part[left, lower, :].astype(F32) + rx[lower, :].astype(F32)
        ).astype(BF16)
        tp_copy(part.at[left, lower], fr.at[lower], rs_s.at[0], rs_r.at[2, k], left).start()

    def give_back(k):
        start, rows = span(k)
        got(part.at[pl.ds(0, 2), pl.ds(start, rows)], rs_r.at[2, k])
        whole = pl.ds(start, rows)
        ret[whole, :] = (
            part[tp, whole, :].astype(F32) + fl[whole, :].astype(F32) + fr[whole, :].astype(F32)
        ).astype(BF16)
        for r in PIECES[k]:
            if r == 0:
                ret_in[0:cap, :] = ret[0:cap, :]
            exchange(
                lambda at: ret.at[at],
                lambda at: ret_in.at[at],
                ret_s.at[0],
                ret_r.at[k],
                r,
                -1,
            )

    def combine(k):
        got(ret_in.at[crossed(PIECES[k])], ret_r.at[k])
        start, rows = span(k)
        picks = [[], []]
        for r in PIECES[k]:
            slot = slots_of(r, (tokens, sizes[r]), 1)
            for i in range(2):
                picks[i].append((slot == cols8[:, 1 + i : 2 + i]).astype(F32))
        routed = hid[...]
        for i in range(2):
            pick = jnp.concatenate(picks[i], axis=1).astype(BF16)
            routed = routed + cols8[:, 3 + i : 4 + i] * jnp.dot(
                pick, ret_in[start : start + rows, :], preferred_element_type=F32
            )
        hid[...] = routed

    def all_gone():
        slots = xin.shape[1]
        near_rows = sum(sizes[:NEAR])
        got(mix.at[pl.ds(0, ntp - 1)], mix_s.at[0])
        got(gains.at[pl.ds(0, ntp - 1)], mix_s.at[1])
        got(outgo.at[pl.ds(near_rows, slots - near_rows)], disp_s.at[0])
        got(outrow.at[:, pl.ds(cap, near_rows - cap)], disp_s.at[1])
        got(ret.at[pl.ds(cap, slots - cap)], ret_s.at[0])
        got(part.at[pl.ds(0, ntp - 1)], rs_s.at[0])
        got(xin.at[pl.ds(0, ntp - 1), pl.ds(0, slots - near_rows + tokens)], ag_s.at[0])

    steps = {
        "own": own,
        "forward": forward,
        "rest": rest,
        "up": lambda k: (arrived(k), experts_up(*span(k))),
        "down": lambda k: experts_down(*span(k)),
        "add": reduce_add,
        "back": give_back,
        "combine": combine,
        "tokens": lambda k: ring_forward(tok, 0, tokens, RING),
        "near": lambda k: near(),
        "weights": lambda k: [loads[i].wait() for i in range(11, 14)],
        "start": reduce_start,
        "gone": lambda k: all_gone(),
    }
    for name, k in ORDER:
        with jax.named_scope(f"{name}{k}"):
            steps[name](k)
    with jax.named_scope("out"):
        out_ref[...] = hid[...].astype(BF16)

def per_device(
    residual_in,
    conv_input,
    outer_gate,
    inner_gate,
    documents,
    conv_taps,
    mixer_gain,
    output_weight,
    ffn_gain,
    routes,
    route_weights,
    expert_gate,
    expert_up,
    expert_down,
):
    nsp = lax.axis_size("sp")
    ntp = lax.axis_size("tp")
    tokens, features = residual_in.shape
    channels = conv_input.shape[1]
    cap = 4 * tokens // nsp
    slots = nsp * cap
    sizes = [count * cap for _, _, count in REGIONS]
    largest = max(sum(sizes[r] for r in piece) for piece in PIECES)
    width = features * ntp
    hidden_units = expert_gate.shape[2]
    args = (
        residual_in,
        conv_input,
        outer_gate,
        inner_gate,
        documents.reshape(1, tokens),
        conv_taps,
        mixer_gain.reshape(1, -1),
        output_weight,
        ffn_gain.reshape(1, -1),
        routes.T,
        route_weights.T,
        expert_gate,
        expert_up,
        expert_down,
    )
    locals_ = [
        pltpu.VMEM(a.shape if a.ndim == 2 else a.shape[1:], a.dtype) for a in args
    ]
    dma = pltpu.SemaphoreType.DMA
    scratch = locals_ + [
        pltpu.VMEM((8, tokens), F32),
        pltpu.VMEM((tokens, 8), F32),
        pltpu.VMEM((tokens + 8, channels), F32),
        pltpu.VMEM((tokens + 8, channels), F32),
        pltpu.VMEM((16, channels), F32),
        pltpu.VMEM((16, channels), F32),
        pltpu.VMEM((ntp, 1, features), F32),
        pltpu.VMEM((ntp, tokens, channels), BF16),
        pltpu.VMEM((ntp, tokens, features), BF16),
        pltpu.VMEM((tokens, features), F32),
        pltpu.VMEM((slots, tokens), BF16),
        pltpu.VMEM((slots, features), BF16),
        pltpu.VMEM((ntp, sum(sizes[:NEAR]), features), BF16),
        pltpu.VMEM((ntp, slots, features), BF16),
        pltpu.VMEM((largest, 128), F32),
        pltpu.VMEM((largest, hidden_units), BF16),
        pltpu.VMEM((ntp, slots, features), BF16),
        pltpu.VMEM((slots, features), BF16),
        pltpu.VMEM((slots, features), BF16),
        pltpu.VMEM((slots, features), BF16),
        pltpu.VMEM((slots, features), BF16),
        pltpu.VMEM((slots, features), BF16),
        dma((len(args),)),
        dma((2,)),
        dma((2,)),
        dma((2,)),
        dma((2,)),
        dma((RING + 2,)),
        dma((1,)),
        dma((3, RING + 1)),
        dma((1,)),
        dma((3, len(PIECES))),
        dma((1,)),
        dma((len(PIECES),)),
        pltpu.SemaphoreType.REGULAR((3,)),
    ]
    return pl.pallas_call(
        functools.partial(layer_kernel, nsp, ntp, cap),
        out_shape=jax.ShapeDtypeStruct((tokens, features), BF16),
        in_specs=[pl.BlockSpec(memory_space=pl.ANY)] * len(args),
        out_specs=pl.BlockSpec(memory_space=pltpu.VMEM),
        scratch_shapes=scratch,
        compiler_params=pltpu.CompilerParams(
            collective_id=0, has_side_effects=True, vmem_limit_bytes=60 * 1024 * 1024
        ),
        cost_estimate=pl.CostEstimate(
            flops=6 * nsp * cap * width * hidden_units,
            bytes_accessed=6 * width * hidden_units,
            transcendentals=0,
        ),
        name="layer",
    )(*args)


def solution(mesh):
    placed = (
        P("sp", "tp"),
        P("sp", "tp"),
        P("sp", "tp"),
        P("sp", "tp"),
        P("sp"),
        P(None, "tp"),
        P(),
        P(None, "tp"),
        P("tp"),
        P("sp", None),
        P("sp", None),
        P("sp", None, "tp"),
        P("sp", None, "tp"),
        P("sp", "tp", None),
    )
    return jax.shard_map(
        per_device, mesh=mesh, in_specs=placed, out_specs=P("sp", "tp"), check_vma=False
    )
```

```python
import functools

import jax
import jax.numpy as jnp
from jax import lax
from jax.experimental import pallas as pl
from jax.experimental.pallas import tpu as pltpu
from jax.sharding import PartitionSpec as P

EPS = 1e-06
CORES = 2
NX = 4
REGIONS = (
    (0, 0, 8),
    (1, 0, 8),
    (-1, 0, 8),
    (2, 0, 4),
    (-2, 0, 4),
    (2, 4, 4),
    (-2, 4, 4),
    (3, 0, 4),
    (-3, 0, 4),
    (3, 4, 4),
    (-3, 4, 4),
    (4, 0, 8),
)
NEAR = 3
RINGS = ((3, 4), (5, 6), (7, 8), (9, 10), (11,))
RING = len(RINGS)
PIECES = ((3, 4), (5, 6), (7, 8, 9, 10), (11,), (1, 2), (0,))
ORDER = (
    ("tokens", 0),
    ("own", 0),
    ("near", 0),
    ("forward", 0),
    ("own", 1),
    ("own", 2),
    ("forward", 1),
    ("weights", 0),
    ("rest", 0),
    ("up", 0),
    ("down", 0),
    ("start", 0),
    ("forward", 2),
    ("own", 3),
    ("rest", 1),
    ("up", 1),
    ("down", 1),
    ("start", 1),
    ("forward", 3),
    ("own", 4),
    ("add", 0),
    ("up", 5),
    ("down", 5),
    ("add", 1),
    ("rest", 2),
    ("rest", 3),
    ("up", 2),
    ("forward", 4),
    ("down", 2),
    ("start", 2),
    ("back", 0),
    ("back", 1),
    ("rest", 4),
    ("up", 3),
    ("add", 2),
    ("down", 3),
    ("start", 3),
    ("start", 5),
    ("up", 4),
    ("down", 4),
    ("back", 2),
    ("add", 3),
    ("start", 4),
    ("add", 5),
    ("back", 3),
    ("combine", 0),
    ("combine", 1),
    ("add", 4),
    ("back", 5),
    ("back", 4),
    ("combine", 2),
    ("combine", 3),
    ("combine", 5),
    ("combine", 4),
    ("gone", 0),
)
MESH = pl.DeviceIdType.MESH
F32 = jnp.float32
BF16 = jnp.bfloat16


def layer_kernel(
    nsp,
    ntp,
    cap,
    res_h,
    ci_h,
    og_h,
    ig_h,
    doc_h,
    taps_h,
    mg_h,
    ow_h,
    fg_h,
    rt_h,
    rw_h,
    wg_h,
    wu_h,
    wd_h,
    out_ref,
    res,
    ci,
    og,
    ig,
    doc,
    taps,
    mg,
    ow,
    fg,
    rt,
    rw,
    wg,
    wu,
    wd,
    rows8,
    cols8,
    joined,
    docj,
    halo_out,
    halo_in,
    gains,
    mix,
    tok,
    hid,
    perm,
    outgo,
    outrow,
    xin,
    scl,
    act,
    part,
    rx,
    fl,
    fr,
    ret,
    ret_in,
    load_sem,
    halo_sem,
    mix_s,
    mix_r,
    disp_s,
    disp_r,
    ag_s,
    ag_r,
    rs_s,
    rs_r,
    ret_s,
    ret_r,
    round_sem,
):
    sp = lax.axis_index("sp")
    tp = lax.axis_index("tp")
    nz = nsp // (NX * CORES)
    zpos = sp // (NX * CORES)
    xpos = (sp // CORES) % NX
    cpos = sp % CORES
    tokens, features = res.shape
    channels = ci.shape[1]
    peers = NX * CORES
    plane = peers * cap
    mine = xpos * CORES + cpos
    base, most = [], 0
    for _, _, count in REGIONS:
        base.append(most)
        most += count * cap
    sizes = [count * cap for _, _, count in REGIONS]
    left = lax.rem(tp + ntp - 1, ntp)
    right = lax.rem(tp + 1, ntp)
    opposite = lax.rem(tp + 2, ntp)

    def along_z(dz):
        return lax.rem(zpos + (dz + nz), nz) * peers + mine

    def signal(sem, to):
        pl.semaphore_signal(sem, inc=1, device_id=to, device_id_type=MESH)

    barrier = pltpu.get_barrier_semaphore()
    for d in range(1, ntp):
        signal(barrier, (sp, lax.rem(tp + d, ntp)))
    for d in (1, nsp - 1):
        signal(barrier, (lax.rem(sp + d, nsp), tp))
    for d in range(1, peers):
        signal(barrier, (zpos * peers + lax.rem(mine + d, peers), tp))
    for d in (1, -1, 2, -2):
        signal(barrier, (along_z(d), tp))
    greeted = ntp - 1 + 2 + peers - 1 + 4

    pairs = (
        (rt_h, rt),
        (doc_h, doc),
        (rw_h, rw),
        (ci_h, ci),
        (ig_h, ig),
        (og_h, og),
        (taps_h, taps),
        (fg_h, gains.at[tp]),
        (mg_h, mg),
        (ow_h, ow),
        (res_h, res),
        (wg_h.at[0], wg),
        (wu_h.at[0], wu),
        (wd_h.at[0], wd),
    )
    loads = [
        pltpu.make_async_copy(src, dst, load_sem.at[i]) for i, (src, dst) in enumerate(pairs)
    ]
    for load in loads:
        load.start()

    for i in (1, 3, 4, 5, 6, 7):
        loads[i].wait()
    docs = jnp.transpose(jnp.broadcast_to(doc[...].astype(F32), (8, tokens)))[:, 0:1]
    value = (ig[...].astype(F32) * ci[...].astype(F32)).astype(BF16).astype(F32)
    joined[8:, :] = value
    docj[8:, :] = jnp.broadcast_to(docs, (tokens, channels))
    halo_out[0:8, :] = value[tokens - 8 :, :]
    halo_out[8:16, :] = docj[tokens : tokens + 8, :]

    def convolve(lo, hi):
        docs_now = docj[8 + lo : 8 + hi, :]
        same_one = (docj[7 + lo : 7 + hi, :] == docs_now).astype(F32)
        same_two = (docj[6 + lo : 6 + hi, :] == docs_now).astype(F32)
        conv_sum = (
            taps[2:3, :] * joined[8 + lo : 8 + hi, :]
            + taps[1:2, :] * joined[7 + lo : 7 + hi, :] * same_one
            + taps[0:1, :] * joined[6 + lo : 6 + hi, :] * same_two
        )
        mix[tp, lo:hi, :] = (og[lo:hi, :].astype(F32) * conv_sum).astype(BF16)

    def to_tp(ref, send, recv):
        for d in (2, 1, ntp - 1):
            pltpu.make_async_remote_copy(
                src_ref=ref,
                dst_ref=ref,
                send_sem=send,
                recv_sem=recv,
                device_id=(sp, lax.rem(tp + d, ntp)),
                device_id_type=MESH,
            ).start()

    def got(ref, sem):
        with jax.named_scope("wait"):
            pltpu.make_async_copy(ref, ref, sem).wait()

    edge = 16
    convolve(edge, tokens)
    with jax.named_scope("barrier"):
        pl.semaphore_wait(barrier, greeted)
    halo = pltpu.make_async_remote_copy(
        src_ref=halo_out,
        dst_ref=halo_in,
        send_sem=halo_sem.at[0],
        recv_sem=halo_sem.at[1],
        device_id=(lax.rem(sp + 1, nsp), tp),
        device_id_type=MESH,
    )
    halo.start()
    for d in (2, -2):
        signal(round_sem.at[0], (along_z(d), tp))
    to_tp(mix.at[tp, pl.ds(edge, tokens - edge)], mix_s.at[0], mix_r.at[0])
    to_tp(gains.at[tp], mix_s.at[1], mix_r.at[1])

    loads[0].wait()
    loads[2].wait()
    experts_iota = lax.broadcasted_iota(jnp.int32, (nsp, tokens), 0)
    first = (experts_iota == rt[0:1, :]).astype(F32)
    second = (experts_iota == rt[1:2, :]).astype(F32)
    named = (first + second).astype(BF16)
    before = (
        lax.broadcasted_iota(jnp.int32, (tokens, tokens), 0)
        < lax.broadcasted_iota(jnp.int32, (tokens, tokens), 1)
    ).astype(F32).astype(BF16)
    earlier = jnp.dot(named, before, preferred_element_type=F32)
    slots = earlier + (experts_iota * cap).astype(F32)
    rows8[0:1, :] = doc[...].astype(F32)
    rows8[1:2, :] = jnp.sum(first * slots, axis=0, keepdims=True)
    rows8[2:3, :] = jnp.sum(second * slots, axis=0, keepdims=True)
    rows8[3:5, :] = rw[...]
    rows8[5:8, :] = jnp.zeros((3, tokens), F32)
    cols8[...] = jnp.transpose(rows8[...])

    def slots_of(r, shape, dim):
        dz, skip, _ = REGIONS[r]
        line = lax.broadcasted_iota(jnp.int32, shape, dim)
        peer = lax.rem(line // cap + (mine + skip), peers)
        zz = lax.rem(zpos + (dz + nz), nz)
        return (zz * plane + peer * cap + lax.rem(line, cap)).astype(F32)

    for r in range(len(REGIONS)):
        slot = slots_of(r, (sizes[r], tokens), 0)
        hit = (slot == rows8[1:2, :]) | (slot == rows8[2:3, :])
        perm[base[r] : base[r] + sizes[r], :] = hit.astype(F32).astype(BF16)

    with jax.named_scope("halowait"):
        halo.wait()
    joined[0:8, :] = halo_in[0:8, :]
    docj[0:8, :] = jnp.where(sp == 0, -1.0, halo_in[8:16, :])
    convolve(0, edge)
    to_tp(mix.at[tp, pl.ds(0, edge)], mix_s.at[0], mix_r.at[0])
    pl.semaphore_wait(round_sem.at[0], 2)
    for d in range(1, peers):
        signal(round_sem.at[1], (zpos * peers + lax.rem(mine + d, peers), tp))

    for i in range(8, 11):
        loads[i].wait()
    with jax.named_scope("mixwait"):
        got(mix.at[pl.ds(0, ntp - 1)], mix_r.at[0])
        got(gains.at[pl.ds(0, ntp - 1)], mix_r.at[1])
    pieces = jnp.concatenate([mix[q] for q in range(ntp)], axis=1).astype(F32)
    squares = jnp.sum(pieces * pieces, axis=1, keepdims=True)
    mix_scale = lax.rsqrt(squares / (channels * ntp) + EPS)
    scaled = (pieces * mg[...]).astype(BF16)
    projected = jnp.dot(scaled, ow[...], preferred_element_type=F32)
    hidden = res[...].astype(F32) + projected * mix_scale
    hid[...] = hidden
    gained = (hidden * gains[tp]).astype(BF16)
    tok[tp] = gained

    def tp_copy(src, dst, send, recv, to):
        return pltpu.make_async_remote_copy(
            src_ref=src,
            dst_ref=dst,
            send_sem=send,
            recv_sem=recv,
            device_id=(sp, to),
            device_id_type=MESH,
        )

    def ring_own(buffer, start, rows, k):
        half = rows // 2
        upper = buffer.at[tp, pl.ds(start, half)]
        lower = buffer.at[tp, pl.ds(start + half, half)]
        tp_copy(upper, upper, ag_s.at[0], ag_r.at[0, k], right).start()
        tp_copy(lower, lower, ag_s.at[0], ag_r.at[1, k], left).start()
        tp_copy(lower, lower, ag_s.at[0], ag_r.at[2, k], right).start()
        tp_copy(upper, upper, ag_s.at[0], ag_r.at[2, k], left).start()

    def ring_forward(buffer, start, rows, k):
        half = rows // 2
        upper = buffer.at[left, pl.ds(start, half)]
        lower = buffer.at[right, pl.ds(start + half, half)]
        got(upper, ag_r.at[0, k])
        tp_copy(upper, upper, ag_s.at[0], ag_r.at[2, k], right).start()
        got(lower, ag_r.at[1, k])
        tp_copy(lower, lower, ag_s.at[0], ag_r.at[2, k], left).start()

    def ring_rest(buffer, start, rows, k):
        got(buffer.at[pl.ds(0, 2), pl.ds(start, rows)], ag_r.at[2, k])

    ring_own(tok, 0, tokens, RING)
    with jax.named_scope("roundwait"):
        pl.semaphore_wait(round_sem.at[1], peers - 1)

    def exchange(src, dst, send, recv, regions, way):
        def one(r, i):
            dz, skip, _ = REGIONS[r]
            zz = lax.rem(zpos + (way * dz + nz), nz)
            at = pl.ds(pl.multiple_of(base[r] + i * cap, cap), cap)
            to = lax.rem(mine + way * (i + skip) + peers, peers)
            pltpu.make_async_remote_copy(
                src_ref=src(at),
                dst_ref=dst(at),
                send_sem=send,
                recv_sem=recv(r),
                device_id=(zz * peers + to, tp),
                device_id_type=MESH,
            ).start()

        count = REGIONS[regions[0]][2]

        def turn(i, carry):
            for r in regions:
                one(r, i if way > 0 else count - i)
            return carry

        others = [r for r in regions if r != 0]
        if way > 0:
            for r in others:
                one(r, 0)
        lax.fori_loop(1, count, turn, 0)
        if way < 0:
            for r in others:
                one(r, 0)

    ring_of = {r: g for g, regions in enumerate(RINGS) for r in regions}

    def extent(regions):
        return base[regions[0]], sum(sizes[r] for r in regions)

    def crossed(regions):
        start, rows = extent(regions)
        skip = cap if 0 in regions else 0
        return pl.ds(start + skip, rows - skip)

    def rows_at(r):
        return slice(base[r], base[r] + sizes[r])

    for g, regions in enumerate(RINGS):
        for r in regions:
            outgo[rows_at(r), :] = jnp.dot(
                perm[rows_at(r), :], gained, preferred_element_type=F32
            ).astype(BF16)
        exchange(
            lambda at: outgo.at[at],
            lambda at: xin.at[tp, at],
            disp_s.at[0],
            lambda r: disp_r.at[ring_of[r]],
            regions,
            1,
        )

    def near():
        ring_rest(tok, 0, tokens, RING)
        for q in range(ntp):
            for r in range(NEAR):
                outrow[q, rows_at(r), :] = jnp.dot(
                    perm[rows_at(r), :], tok[q], preferred_element_type=F32
                ).astype(BF16)
            xin[q, 0:cap, :] = outrow[q, 0:cap, :]
        exchange(
            lambda at: outrow.at[:, at],
            lambda at: xin.at[:, at],
            disp_s.at[1],
            lambda r: disp_r.at[RING + min(r, 1)],
            tuple(range(NEAR)),
            1,
        )

    def span(k):
        return extent(PIECES[k])

    def arrived(k):
        if PIECES[k][0] < NEAR:
            got(xin.at[:, crossed(PIECES[k])], disp_r.at[RING + min(PIECES[k][0], 1)])

    def own(g):
        got(xin.at[tp, crossed(RINGS[g])], disp_r.at[g])
        ring_own(xin, *extent(RINGS[g]), g)

    def forward(g):
        ring_forward(xin, *extent(RINGS[g]), g)

    def rest(g):
        ring_rest(xin, *extent(RINGS[g]), g)

    width = features * ntp
    hidden_units = wg.shape[1]
    tile = 128
    wide = 256

    def experts_scale(start, rows):
        total = jnp.zeros((rows, tile), F32)
        for q in range(ntp):
            weight = 1.0 / (gains[q] * gains[q])
            for c in range(features // tile):
                cut = slice(c * tile, (c + 1) * tile)
                x = xin[q, start : start + rows, cut].astype(F32)
                total = total + x * x * weight[:, cut]
        scale = lax.rsqrt(jnp.sum(total, axis=1, keepdims=True) / width + EPS)
        scl[0:rows, :] = jnp.broadcast_to(scale, (rows, tile))

    def experts_up(start, rows):
        def up_tile(n, carry):
            at = pl.ds(pl.multiple_of(n * tile, tile), tile)
            x = jnp.concatenate([xin[q, start : start + rows] for q in range(ntp)], axis=1)
            both = jnp.concatenate([wg[:, at], wu[:, at]], axis=1)
            made = jnp.dot(x, both, preferred_element_type=F32)
            gate = made[:, :tile] * scl[0:rows, :]
            act[0:rows, at] = (
                jax.nn.silu(gate) * (made[:, tile:] * scl[0:rows, :])
            ).astype(BF16)
            return carry

        lax.fori_loop(0, hidden_units // tile, up_tile, 0)

    def experts_down(start, rows):
        for q in range(ntp):
            for k in range(features // wide):
                cols = slice(q * features + k * wide, q * features + (k + 1) * wide)
                part[q, start : start + rows, k * wide : (k + 1) * wide] = jnp.dot(
                    act[0:rows, :], wd[:, cols], preferred_element_type=F32
                ).astype(BF16)

    def reduce_start(k):
        start, rows = span(k)
        half = rows // 2
        upper = pl.ds(start, half)
        lower = pl.ds(start + half, half)
        tp_copy(part.at[opposite, upper], rx.at[upper], rs_s.at[0], rs_r.at[0, k], right).start()
        tp_copy(part.at[opposite, lower], rx.at[lower], rs_s.at[0], rs_r.at[1, k], left).start()
        tp_copy(part.at[right, lower], fl.at[lower], rs_s.at[0], rs_r.at[2, k], right).start()
        tp_copy(part.at[left, upper], fr.at[upper], rs_s.at[0], rs_r.at[2, k], left).start()

    def reduce_add(k):
        start, rows = span(k)
        half = rows // 2
        upper = pl.ds(start, half)
        lower = pl.ds(start + half, half)
        got(rx.at[upper], rs_r.at[0, k])
        part[right, upper, :] = (
            part[right, upper, :].astype(F32) + rx[upper, :].astype(F32)
        ).astype(BF16)
        tp_copy(part.at[right, upper], fl.at[upper], rs_s.at[0], rs_r.at[2, k], right).start()
        got(rx.at[lower], rs_r.at[1, k])
        part[left, lower, :] = (
            part[left, lower, :].astype(F32) + rx[lower, :].astype(F32)
        ).astype(BF16)
        tp_copy(part.at[left, lower], fr.at[lower], rs_s.at[0], rs_r.at[2, k], left).start()

    def give_back(k):
        start, rows = span(k)
        got(part.at[pl.ds(0, 2), pl.ds(start, rows)], rs_r.at[2, k])
        whole = pl.ds(start, rows)
        ret[whole, :] = (
            part[tp, whole, :].astype(F32) + fl[whole, :].astype(F32) + fr[whole, :].astype(F32)
        ).astype(BF16)
        if 0 in PIECES[k]:
            ret_in[0:cap, :] = ret[0:cap, :]
        exchange(
            lambda at: ret.at[at],
            lambda at: ret_in.at[at],
            ret_s.at[0],
            lambda r: ret_r.at[k],
            PIECES[k],
            -1,
        )

    def combine(k):
        got(ret_in.at[crossed(PIECES[k])], ret_r.at[k])
        start, rows = span(k)
        picks = [[], []]
        for r in PIECES[k]:
            slot = slots_of(r, (tokens, sizes[r]), 1)
            for i in range(2):
                picks[i].append((slot == cols8[:, 1 + i : 2 + i]).astype(F32))
        routed = hid[...]
        for i in range(2):
            pick = jnp.concatenate(picks[i], axis=1).astype(BF16)
            routed = routed + cols8[:, 3 + i : 4 + i] * jnp.dot(
                pick, ret_in[start : start + rows, :], preferred_element_type=F32
            )
        hid[...] = routed

    def all_gone():
        slots = xin.shape[1]
        near_rows = sum(sizes[:NEAR])
        got(mix.at[pl.ds(0, ntp - 1)], mix_s.at[0])
        got(gains.at[pl.ds(0, ntp - 1)], mix_s.at[1])
        got(outgo.at[pl.ds(near_rows, slots - near_rows)], disp_s.at[0])
        got(outrow.at[:, pl.ds(cap, near_rows - cap)], disp_s.at[1])
        got(ret.at[pl.ds(cap, slots - cap)], ret_s.at[0])
        got(part.at[pl.ds(0, ntp - 1)], rs_s.at[0])
        got(xin.at[pl.ds(0, ntp - 1), pl.ds(0, slots - near_rows + tokens)], ag_s.at[0])

    steps = {
        "own": own,
        "forward": forward,
        "rest": rest,
        "up": lambda k: (arrived(k), experts_scale(*span(k)), experts_up(*span(k))),
        "down": lambda k: experts_down(*span(k)),
        "add": reduce_add,
        "back": give_back,
        "combine": combine,
        "tokens": lambda k: ring_forward(tok, 0, tokens, RING),
        "near": lambda k: near(),
        "weights": lambda k: [loads[i].wait() for i in range(11, 14)],
        "start": reduce_start,
        "gone": lambda k: all_gone(),
    }
    for name, k in ORDER:
        with jax.named_scope(f"{name}{k}"):
            steps[name](k)
    with jax.named_scope("out"):
        out_ref[...] = hid[...].astype(BF16)

def per_device(
    residual_in,
    conv_input,
    outer_gate,
    inner_gate,
    documents,
    conv_taps,
    mixer_gain,
    output_weight,
    ffn_gain,
    routes,
    route_weights,
    expert_gate,
    expert_up,
    expert_down,
):
    nsp = lax.axis_size("sp")
    ntp = lax.axis_size("tp")
    tokens, features = residual_in.shape
    channels = conv_input.shape[1]
    cap = 4 * tokens // nsp
    slots = nsp * cap
    sizes = [count * cap for _, _, count in REGIONS]
    largest = max(sum(sizes[r] for r in piece) for piece in PIECES)
    width = features * ntp
    hidden_units = expert_gate.shape[2]
    args = (
        residual_in,
        conv_input,
        outer_gate,
        inner_gate,
        documents.reshape(1, tokens),
        conv_taps,
        mixer_gain.reshape(1, -1),
        output_weight,
        ffn_gain.reshape(1, -1),
        routes.T,
        route_weights.T,
        expert_gate,
        expert_up,
        expert_down,
    )
    locals_ = [
        pltpu.VMEM(a.shape if a.ndim == 2 else a.shape[1:], a.dtype) for a in args
    ]
    dma = pltpu.SemaphoreType.DMA
    scratch = locals_ + [
        pltpu.VMEM((8, tokens), F32),
        pltpu.VMEM((tokens, 8), F32),
        pltpu.VMEM((tokens + 8, channels), F32),
        pltpu.VMEM((tokens + 8, channels), F32),
        pltpu.VMEM((16, channels), F32),
        pltpu.VMEM((16, channels), F32),
        pltpu.VMEM((ntp, 1, features), F32),
        pltpu.VMEM((ntp, tokens, channels), BF16),
        pltpu.VMEM((ntp, tokens, features), BF16),
        pltpu.VMEM((tokens, features), F32),
        pltpu.VMEM((slots, tokens), BF16),
        pltpu.VMEM((slots, features), BF16),
        pltpu.VMEM((ntp, sum(sizes[:NEAR]), features), BF16),
        pltpu.VMEM((ntp, slots, features), BF16),
        pltpu.VMEM((largest, 128), F32),
        pltpu.VMEM((largest, hidden_units), BF16),
        pltpu.VMEM((ntp, slots, features), BF16),
        pltpu.VMEM((slots, features), BF16),
        pltpu.VMEM((slots, features), BF16),
        pltpu.VMEM((slots, features), BF16),
        pltpu.VMEM((slots, features), BF16),
        pltpu.VMEM((slots, features), BF16),
        dma((len(args),)),
        dma((2,)),
        dma((2,)),
        dma((2,)),
        dma((2,)),
        dma((RING + 2,)),
        dma((1,)),
        dma((3, RING + 1)),
        dma((1,)),
        dma((3, len(PIECES))),
        dma((1,)),
        dma((len(PIECES),)),
        pltpu.SemaphoreType.REGULAR((2,)),
    ]
    return pl.pallas_call(
        functools.partial(layer_kernel, nsp, ntp, cap),
        out_shape=jax.ShapeDtypeStruct((tokens, features), BF16),
        in_specs=[pl.BlockSpec(memory_space=pl.ANY)] * len(args),
        out_specs=pl.BlockSpec(memory_space=pltpu.VMEM),
        scratch_shapes=scratch,
        compiler_params=pltpu.CompilerParams(
            collective_id=0, has_side_effects=True, vmem_limit_bytes=60 * 1024 * 1024
        ),
        cost_estimate=pl.CostEstimate(
            flops=6 * nsp * cap * width * hidden_units,
            bytes_accessed=6 * width * hidden_units,
            transcendentals=0,
        ),
        name="layer",
    )(*args)


def solution(mesh):
    placed = (
        P("sp", "tp"),
        P("sp", "tp"),
        P("sp", "tp"),
        P("sp", "tp"),
        P("sp"),
        P(None, "tp"),
        P(),
        P(None, "tp"),
        P("tp"),
        P("sp", None),
        P("sp", None),
        P("sp", None, "tp"),
        P("sp", None, "tp"),
        P("sp", "tp", None),
    )
    return jax.shard_map(
        per_device, mesh=mesh, in_specs=placed, out_specs=P("sp", "tp"), check_vma=False
    )
```
